32 devices in a mesh: grp: 2 (over y), sp: 4 (over z), tp: 4 (over x, core).
Axes of the slice: x: 2, y: 2, z: 4, core: 2. Of those that a mesh axis runs over, the one named last changes fastest.
Arguments:
- queries: bfloat16 [4096, 1024], P(('grp', 'sp'), 'tp'), parts along dimension 0, may hold values from -120 to 120
- keys: bfloat16 [4096, 256], P(('grp', 'sp')), parts along dimension 0, may hold values from -6 to 6
- values: bfloat16 [4096, 256], P(('grp', 'sp')), parts along dimension 0, may hold values from -6 to 6
- sink: float32 [8], P('tp'), may hold values from 1 to 5
- resid: bfloat16 [4096, 2048], P(('grp', 'sp')), parts along dimension 0, may hold values from -100 to 100
- out_proj: bfloat16 [1024, 2048], P(None, 'tp'), may hold values from -1.5 to 1.5
- norm_gain: float32 [2048], replicated, may hold values from 0.1 to 1.9
- w_gate: bfloat16 [2048, 6144], P('sp', 'tp'), may hold values from -0.125 to 0.125
- w_up: bfloat16 [2048, 6144], P('sp', 'tp'), may hold values from -0.125 to 0.125
- conv_w: float32 [3, 6144], P(None, 'tp'), may hold values from -3 to 3
- conv_b: float32 [6144], P('tp'), may hold values from -3 to 3
- w_down: bfloat16 [6144, 2048], P('tp', 'sp'), may hold values from -0.21875 to 0.21875
Outputs:
- layer_out: bfloat16 [4096, 2048], P(('grp', 'sp'), 'tp'), parts along dimension 0
The draws below stay inside these ranges and needn't reach their ends.
There are 2 independent parts, one for each index of `grp`. The reference program is written for one: setup_inputs(seed, part) draws one part's arguments, and reference() takes and returns one part's arrays. A program takes and returns all parts, laid end to end along the dimension named above; an argument that names none is the same for every part. Nothing has to cross between parts.
All inputs are finite; a program needn't handle non-finite values.
Results may differ from the reference program's by a relative error of at most 0.015.
Values may be sent and summed in bfloat16 or wider, within the bound.
A program may use at most 64 MiB of HBM per device.

```python
import jax
import jax.numpy as jnp
from jax import lax

D = 2048
FF = 6144
H = 8
KVH = 2
HD = 128
WINDOW = 128
CONV = 3
TOK_DEV = 512
SEQ = 2048


def joint_qk(key):
    base = jax.random.fold_in(key, 11)
    key_q, key_k = jax.random.split(base)
    q_vals = jnp.clip(jax.random.normal(key_q, (SEQ, H, HD), jnp.float32), -6.0, 6.0)
    k_vals = jnp.clip(jax.random.normal(key_k, (SEQ, KVH, HD), jnp.float32), -6.0, 6.0)
    return (q_vals.reshape(SEQ, H * HD), k_vals.reshape(SEQ, KVH * HD))


def draw_queries(key, part):
    return joint_qk(key)[0].astype(jnp.bfloat16)


def draw_keys(key, part):
    return joint_qk(key)[1].astype(jnp.bfloat16)


def draw_resid(key, part):
    base = jax.random.fold_in(key, 23)
    key_n, key_r, key_c = jax.random.split(base, 3)
    trend = 0.5 + jnp.arange(D, dtype=jnp.float32) / D
    columns = jnp.exp(jax.random.uniform(key_c, (D,), jnp.float32, -0.7, 0.7)) * trend
    noise = jnp.clip(jax.random.normal(key_n, (SEQ, D), jnp.float32), -6.0, 6.0)
    rows = jnp.exp(jax.random.uniform(key_r, (SEQ, 1), jnp.float32, -0.69, 1.6))
    return jnp.clip(noise * rows * columns[None, :], -100.0, 100.0).astype(jnp.bfloat16)


def spiked(array, key, source, target, blocks, factor):
    def block_of(dim):
        return (jnp.arange(array.shape[dim]) // (array.shape[dim] // blocks)).reshape((-1,) + (1,) * (array.ndim - 1 - dim))

    first = jax.random.permutation(key, blocks)[block_of(target)]
    other_side = (block_of(target) + blocks // 2) % blocks
    return jnp.where((block_of(source) == first) | (block_of(source) == other_side), factor * array, array)


def steps_of(own_key, dims, cuts, least, high):
    loudness, own = 1.0, jax.random.fold_in(own_key, 6)
    for dim, parts in cuts:
        draws = jnp.exp(jax.random.uniform(jax.random.fold_in(own, dim), (parts,), jnp.float32, least / len(cuts), high / len(cuts)))
        loudness = loudness * jnp.repeat(draws, dims[dim] // parts).reshape([-1 if axis == dim else 1 for axis in range(len(dims))])
    return loudness


def gaussian(key, shape, scale, most, cuts=(), kind=jnp.bfloat16):
    drawn = scale * jax.random.normal(key, shape, jnp.float32)
    if cuts:
        drawn = drawn * steps_of(key, shape, cuts, -0.22, 0.18)
    return jnp.clip(drawn, -most, most).astype(kind)


def noise_with(own_key, extent, scale, reach, cuts, heavy, held_as=jnp.bfloat16):
    drawn = scale * jax.random.normal(own_key, extent, jnp.float32)
    if cuts:
        drawn = drawn * steps_of(own_key, extent, cuts, -0.22, 0.18)
    return jnp.clip(spiked(drawn, jax.random.fold_in(own_key, 3), *heavy), -reach, reach).astype(held_as)


def setup_inputs(seed: int = 0, part: int = 0) -> dict:
    key_list = jax.random.split(jax.random.key(seed), 13)
    own_keys = jax.random.split(jax.random.fold_in(key_list[12], part), 13)
    return {
        "queries": draw_queries(jax.random.fold_in(jax.random.fold_in(key_list[12], part), 71), part),
        "keys": draw_keys(jax.random.fold_in(jax.random.fold_in(key_list[12], part), 71), part),
        "values": gaussian(own_keys[2], (SEQ, KVH * HD), 1.0, 6.0, ((0, 4),)),
        "sink": jnp.clip(1.0 + 4.0 * jax.random.uniform(key_list[3], (H,), jnp.float32) ** steps_of(key_list[3], (H,), ((0, 4),), -0.2, 0.2), 1.0, 5.0),
        "resid": draw_resid(jax.random.fold_in(jax.random.fold_in(key_list[12], part), 71), part),
        "out_proj": gaussian(key_list[5], (H * HD, D), (H * HD // 64) ** -0.5, 1.5, ((1, 4),)),
        "norm_gain": jnp.clip(1.0 + 0.18 * jax.random.normal(key_list[6], (D,), jnp.float32), 0.1, 1.9),
        "w_gate": gaussian(key_list[7], (D, FF), D ** -0.5, 0.125, ((0, 4), (1, 4))),
        "w_up": gaussian(key_list[8], (D, FF), D ** -0.5, 0.125, ((0, 4), (1, 4))),
        "conv_w": gaussian(key_list[9], (CONV, FF), 0.6, 3.0, ((1, 4),), jnp.float32),
        "conv_b": gaussian(key_list[10], (FF,), 0.5, 3.0, ((0, 4),), jnp.float32),
        "w_down": noise_with(key_list[11], (FF, D), (FF // 4) ** -0.5, 0.21875, ((0, 4), (1, 4)), (0, 1, 4, 2.0)),
    }


def reference(queries, keys, values, sink, resid, out_proj, norm_gain, w_gate, w_up, conv_w, conv_b, w_down):
    group = H // KVH
    scale = HD ** (-0.5)
    span = TOK_DEV + 2 * WINDOW
    q_heads = queries.reshape(SEQ, H, HD)
    k_pad = jnp.pad(keys.reshape(SEQ, KVH, HD), ((WINDOW, WINDOW), (0, 0), (0, 0)))
    v_pad = jnp.pad(values.reshape(SEQ, KVH, HD), ((WINDOW, WINDOW), (0, 0), (0, 0)))
    sink_grid = sink.reshape(KVH, group)[:, :, None]

    def block(index):
        start = (index * TOK_DEV).astype(jnp.int32)
        q_block = lax.dynamic_slice_in_dim(q_heads, start, TOK_DEV, 0).astype(jnp.float32)
        q_block = q_block.reshape(TOK_DEV, KVH, group, HD)
        k_block = lax.dynamic_slice_in_dim(k_pad, start, span, 0).astype(jnp.float32)
        v_block = lax.dynamic_slice_in_dim(v_pad, start, span, 0).astype(jnp.float32)
        scores = jnp.einsum('qhgd,khd->hgqk', q_block, k_block) * scale
        q_pos = start + jnp.arange(TOK_DEV, dtype=jnp.int32)[:, None]
        k_pos = start - WINDOW + jnp.arange(span, dtype=jnp.int32)[None, :]
        valid = (jnp.abs(q_pos - k_pos) <= WINDOW) & (k_pos >= 0) & (k_pos < SEQ)
        scores = jnp.where(valid, scores, jnp.float32(-1e+30))
        top = jnp.maximum(lax.optimization_barrier(jnp.max(scores, axis=-1)), sink_grid)
        expo = jnp.exp(scores - top[..., None])
        total = lax.optimization_barrier(jnp.sum(expo, axis=-1)) + jnp.exp(sink_grid - top)
        weights = (expo / total[..., None]).astype(jnp.bfloat16)
        out = jnp.einsum('hgqk,khd->qhgd', weights.astype(jnp.float32), v_block)
        return out.astype(jnp.bfloat16).reshape(TOK_DEV, H * HD)
    mixed = lax.map(block, jnp.arange(SEQ // TOK_DEV, dtype=jnp.int32)).reshape(SEQ, H * HD)
    summed = resid.astype(jnp.float32) + jnp.dot(mixed, out_proj, preferred_element_type=jnp.float32)
    mean = lax.optimization_barrier(jnp.mean(summed, axis=-1, keepdims=True))
    msq = lax.optimization_barrier(jnp.mean(summed * summed, axis=-1, keepdims=True))
    normed = ((summed - mean) * lax.rsqrt(msq - mean * mean + 1e-05) * norm_gain).astype(jnp.bfloat16)
    gate_pre = jnp.dot(normed, w_gate, preferred_element_type=jnp.float32).astype(jnp.bfloat16)
    up_part = jnp.dot(normed, w_up, preferred_element_type=jnp.float32).astype(jnp.bfloat16)
    padded = jnp.pad(gate_pre.astype(jnp.float32), ((1, 1), (0, 0)))
    conv = conv_b
    for tap in range(CONV):
        conv = conv + padded[tap:tap + SEQ] * conv_w[tap]
    act = (jax.nn.silu(conv) * up_part.astype(jnp.float32)).astype(jnp.bfloat16)
    ffn = jnp.dot(act, w_down, preferred_element_type=jnp.float32)
    return (normed.astype(jnp.float32) + ffn).astype(jnp.bfloat16)
```

```python
import functools

import jax
import jax.numpy as jnp
from jax import lax
from jax.experimental import pallas as pl
from jax.experimental.pallas import tpu as pltpu
from jax.sharding import PartitionSpec as P

H = 8
KVH = 2
HD = 128
WINDOW = 128
CONV = 3


def with_halo(cells, sides, width):
    for axis, dim in sides:
        count = lax.axis_size(axis)
        ends = count - 1
        head = lax.slice_in_dim(cells, 0, width, axis=dim)
        tail = lax.slice_in_dim(cells, cells.shape[dim] - width, cells.shape[dim], axis=dim)
        cells = jnp.concatenate(
            [
                lax.ppermute(tail, axis, [(i, (i + 1) % count) for i in range(ends)]),
                cells,
                lax.ppermute(head, axis, [((i + 1) % count, i) for i in range(ends)]),
            ],
            axis=dim,
        )
    return cells


def shards(
    queries, keys, values, sink, resid, out_proj, norm_gain, w_gate, w_up, conv_w, conv_b, w_down
):
    tokens = queries.shape[0]
    width = resid.shape[1]
    heads_here = sink.shape[0]
    group = H // KVH
    scale = HD ** (-0.5)
    first_head = lax.axis_index("tp") * heads_here
    kv_head = first_head // group
    own_keys = lax.dynamic_slice_in_dim(keys, kv_head * HD, HD, 1)
    own_values = lax.dynamic_slice_in_dim(values, kv_head * HD, HD, 1)
    extended = with_halo(jnp.stack([own_keys, own_values]), (("sp", 1),), WINDOW)
    ext_keys = extended[0]
    ext_values = extended[1]
    span = tokens + 2 * WINDOW
    q_heads = queries.reshape(tokens, heads_here, HD)
    scores = (
        jnp.einsum("qhd,kd->hqk", q_heads, ext_keys, preferred_element_type=jnp.float32) * scale
    )
    offset = lax.axis_index("sp") * tokens
    q_pos = offset + jnp.arange(tokens, dtype=jnp.int32)[:, None]
    k_pos = offset - WINDOW + jnp.arange(span, dtype=jnp.int32)[None, :]
    seq_total = tokens * lax.axis_size("sp")
    valid = (jnp.abs(q_pos - k_pos) <= WINDOW) & (k_pos >= 0) & (k_pos < seq_total)
    scores = jnp.where(valid[None], scores, jnp.float32(-1e30))
    sink_col = sink[:, None]
    top = jnp.maximum(jnp.max(scores, axis=-1), sink_col)
    expo = jnp.exp(scores - top[..., None])
    total = jnp.sum(expo, axis=-1) + jnp.exp(sink_col - top)
    weights = (expo / total[..., None]).astype(jnp.bfloat16)
    heads_out = jnp.einsum("hqk,kd->qhd", weights, ext_values, preferred_element_type=jnp.float32)
    heads_out = heads_out.astype(jnp.bfloat16).reshape(tokens, heads_here * HD)
    all_heads = lax.all_gather(heads_out, "tp", axis=1, tiled=True)
    cols = width // lax.axis_size("tp")
    col_start = lax.axis_index("tp") * cols
    full_proj = lax.all_gather(out_proj, "tp", axis=1, tiled=True)
    summed = resid.astype(jnp.float32) + jnp.dot(
        all_heads, full_proj, preferred_element_type=jnp.float32
    )
    mean = jnp.mean(summed, axis=-1, keepdims=True)
    msq = jnp.mean(summed * summed, axis=-1, keepdims=True)
    normed_full = ((summed - mean) * lax.rsqrt(msq - mean * mean + 1e-05) * norm_gain).astype(
        jnp.bfloat16
    )
    normed_own = lax.dynamic_slice_in_dim(normed_full, col_start, cols, 1)
    gate_acc = jnp.dot(
        normed_full,
        lax.all_gather(w_gate, "sp", axis=0, tiled=True),
        preferred_element_type=jnp.float32,
    )
    up_acc = jnp.dot(
        normed_full,
        lax.all_gather(w_up, "sp", axis=0, tiled=True),
        preferred_element_type=jnp.float32,
    )
    gate_pre = gate_acc.astype(jnp.bfloat16)
    up_part = up_acc.astype(jnp.bfloat16)
    padded = with_halo(gate_pre, (("sp", 0),), CONV // 2)
    conv = conv_b
    for tap in range(CONV):
        conv = conv + padded[tap : tap + tokens].astype(jnp.float32) * conv_w[tap]
    act = (jax.nn.silu(conv) * up_part.astype(jnp.float32)).astype(jnp.bfloat16)
    terms = jnp.dot(
        act, lax.all_gather(w_down, "sp", axis=1, tiled=True), preferred_element_type=jnp.float32
    )
    ffn_own = lax.psum_scatter(
        terms.astype(jnp.bfloat16), "tp", scatter_dimension=1, tiled=True
    ).astype(jnp.float32)
    return (normed_own.astype(jnp.float32) + ffn_own).astype(jnp.bfloat16)


CHUNKS = 2
PAD = 8
EDGE = 16
BF16 = jnp.bfloat16
F32 = jnp.float32


def layer_kernel(
    sizes,
    q_ref, k_ref, v_ref, sink_ref, resid_ref, proj_ref, gain_ref, wg_ref, wu_ref, cw_ref, cb_ref, wd_ref,
    out_ref,
    kv_ext, proj_all, mixed, summed, normed, wg_all, wu_all, wd_all, gate, up, edge, halo, act, terms, parts,
    halo_send, halo_recv, z_recv, right_send, left_send, y_recv, y_send,
    proj_send, proj_recv, mix_send, mix_recv, edge_send, edge_recv, term_send, term_recv,
):
    groups, n, tps = sizes
    g = lax.axis_index("grp")
    s = lax.axis_index("sp")
    t = lax.axis_index("tp")
    tokens, width = resid_ref.shape
    heads_here = sink_ref.shape[0]
    cols = proj_ref.shape[1]
    depth = wg_ref.shape[0]
    hidden = wg_ref.shape[1]
    has_left, has_right = s > 0, s < n - 1
    own = (wg_ref, wu_ref, wd_ref)
    full = (wg_all, wu_all, wd_all)

    def remote(src, dst, send, recv, to):
        return pltpu.make_async_remote_copy(
            src_ref=src, dst_ref=dst, send_sem=send, recv_sem=recv,
            device_id=to, device_id_type=pl.DeviceIdType.MESH,
        )

    barrier = pltpu.get_barrier_semaphore()

    def greet(to):
        pl.semaphore_signal(barrier, inc=1, device_id=to, device_id_type=pl.DeviceIdType.MESH)

    @pl.when(has_left)
    def _():
        greet({"sp": s - 1})

    @pl.when(has_right)
    def _():
        greet({"sp": s + 1})

    for j in range(1, groups):
        greet({"grp": lax.rem(g + j, groups)})
    for j in range(1, tps):
        greet({"tp": lax.rem(t + j, tps)})

    along = jnp.minimum(s, 1) + jnp.minimum(n - 1 - s, 1)
    pl.semaphore_wait(barrier, along + groups - 1 + tps - 1)

    kv_head = (t * heads_here) // (H // KVH)
    kv_cols = pl.ds(pl.multiple_of(kv_head * HD, HD), HD)

    def halo_copy(i, to_left):
        ref = (k_ref, v_ref)[i]
        if to_left:
            return remote(ref.at[pl.ds(0, WINDOW), kv_cols], kv_ext.at[i, pl.ds(WINDOW + tokens, WINDOW)],
                          halo_send.at[i, 0], halo_recv.at[i, 0], {"sp": s - 1})
        return remote(ref.at[pl.ds(tokens - WINDOW, WINDOW), kv_cols], kv_ext.at[i, pl.ds(0, WINDOW)],
                      halo_send.at[i, 1], halo_recv.at[i, 1], {"sp": s + 1})

    def rows_of(m, part, c):
        step = own[m].shape[0] // (groups * CHUNKS)
        return pl.ds(pl.multiple_of((part * CHUNKS + c) * step, EDGE), step)

    def hop(m, p, c, side, is_own):
        rows = rows_of(m, g, c)
        src = own[m].at[rows] if is_own else full[m].at[p, rows]
        sem = (right_send, left_send)[side].at[m, p, c]
        return remote(src, full[m].at[p, rows], sem, z_recv.at[m, p, c], {"sp": (s + 1, s - 1)[side]})

    def cross(m, p, c, j):
        rows = rows_of(m, g, c)
        return remote(full[m].at[p, rows], full[m].at[p, rows], y_send.at[m, p, c, j],
                      y_recv.at[m, p, c, j], {"grp": lax.rem(g + j, groups)})

    def cross_arrival(m, p, c, j):
        rows = rows_of(m, lax.rem(g + groups - j, groups), c)
        return remote(full[m].at[p, rows], full[m].at[p, rows], y_send.at[m, p, c, j],
                      y_recv.at[m, p, c, j], {"grp": lax.rem(g + j, groups)})

    def proj_copy(j):
        return remote(proj_ref, proj_all.at[t], proj_send.at[j], proj_recv.at[j], {"tp": lax.rem(t + j, tps)})

    def proj_arrival(j):
        return remote(proj_ref, proj_all.at[lax.rem(t + tps - j, tps)], proj_send.at[j], proj_recv.at[j],
                      {"tp": lax.rem(t + j, tps)})

    def mix_copy(j):
        return remote(mixed.at[t], mixed.at[t], mix_send.at[j], mix_recv.at[j], {"tp": lax.rem(t + j, tps)})

    def mix_arrival(j):
        return remote(mixed.at[t], mixed.at[lax.rem(t + tps - j, tps)], mix_send.at[j], mix_recv.at[j],
                      {"tp": lax.rem(t + j, tps)})

    sides = ((has_right, 0), (has_left, 1))

    @pl.when(has_left)
    def _():
        for i in range(2):
            halo_copy(i, True).start()

    @pl.when(has_right)
    def _():
        for i in range(2):
            halo_copy(i, False).start()

    for m in range(3):
        for c in range(CHUNKS):
            for able, side in sides:
                @pl.when(able)
                def _(m=m, c=c, side=side):
                    hop(m, s, c, side, True).start()
    for j in range(1, tps):
        proj_copy(j).start()

    for i, ref in enumerate((k_ref, v_ref)):
        kv_ext[i, pl.ds(WINDOW, tokens), :] = ref[:, kv_cols]

    @pl.when(jnp.logical_not(has_left))
    def _():
        kv_ext[:, pl.ds(0, WINDOW), :] = jnp.zeros((2, WINDOW, HD), BF16)

    @pl.when(jnp.logical_not(has_right))
    def _():
        kv_ext[:, pl.ds(WINDOW + tokens, WINDOW), :] = jnp.zeros((2, WINDOW, HD), BF16)

    @pl.when(has_right)
    def _():
        for i in range(2):
            halo_copy(i, True).wait_recv()

    @pl.when(has_left)
    def _():
        for i in range(2):
            halo_copy(i, False).wait_recv()

    span = 3 * WINDOW
    seq_total = tokens * n

    @pl.loop(0, tokens // WINDOW)
    def _(b):
        start = pl.multiple_of(b * WINDOW, WINDOW)
        row = lax.broadcasted_iota(jnp.int32, (WINDOW, span), 0)
        col = lax.broadcasted_iota(jnp.int32, (WINDOW, span), 1)
        k_pos = s * tokens + start - WINDOW + col
        valid = (jnp.abs(row + WINDOW - col) <= WINDOW) & (k_pos >= 0) & (k_pos < seq_total)
        kb = kv_ext[0, pl.ds(start, span), :]
        vb = kv_ext[1, pl.ds(start, span), :]
        for h in range(heads_here):
            qb = q_ref[pl.ds(start, WINDOW), h * HD:(h + 1) * HD]
            sc = lax.dot_general(qb, kb, (((1,), (1,)), ((), ())), preferred_element_type=F32) * (HD ** -0.5)
            sc = jnp.where(valid, sc, F32(-1e30))
            sink = sink_ref[h]
            top = jnp.maximum(jnp.max(sc, axis=-1, keepdims=True), sink)
            expo = jnp.exp(sc - top)
            total = jnp.sum(expo, axis=-1, keepdims=True) + jnp.exp(sink - top)
            weights = (expo / total).astype(BF16)
            o = jnp.dot(weights, vb, preferred_element_type=F32)
            mixed[t, pl.ds(start, WINDOW), h * HD:(h + 1) * HD] = o.astype(BF16)

    proj_all[t] = proj_ref[...]
    for j in range(1, tps):
        mix_copy(j).start()

    def relay(k):
        for m in range(3):
            for c in range(CHUNKS):
                for side in range(2):
                    p = s - k if side == 0 else s + k
                    here = p >= 0 if side == 0 else p < n
                    able = sides[side][0]

                    @pl.when(here)
                    def _(m=m, c=c, side=side, p=p, able=able):
                        hop(m, p, c, side, False).wait_recv()
                        for j in range(1, groups):
                            cross(m, p, c, j).start()
                        if k < n - 1:
                            @pl.when(able)
                            def _():
                                hop(m, p, c, side, False).start()

    def arrived(m, p):
        for c in range(CHUNKS):
            for j in range(1, groups):
                cross_arrival(m, p, c, j).wait_recv()

    tile = cols

    def gate_up(p, first):
        x = normed[:, pl.ds(pl.multiple_of(p * depth, 128), depth)]

        @pl.loop(0, hidden // tile)
        def _(i):
            at = pl.ds(pl.multiple_of(i * tile, 128), tile)
            a = wg_ref[:, at] if first else wg_all[p, :, at]
            ga = jnp.dot(x, a, preferred_element_type=F32)
            b = wu_ref[:, at] if first else wu_all[p, :, at]
            ub = jnp.dot(x, b, preferred_element_type=F32)
            if first:
                gate[pl.ds(PAD, tokens), at] = ga
                up[:, at] = ub
            else:
                gate[pl.ds(PAD, tokens), at] += ga
                up[:, at] += ub

    def pieces(k, do):
        @pl.loop(0, 2)
        def _(side):
            p = s + (2 * side - 1) * k

            @pl.when((p >= 0) & (p < n))
            def _():
                do(p)

    def gate_up_from(k):
        def do(p):
            arrived(0, p)
            arrived(1, p)
            gate_up(p, False)
        pieces(k, do)

    relay(1)

    for j in range(1, tps):
        proj_arrival(j).wait_recv()
        mix_arrival(j).wait_recv()
    lanes = mixed.shape[2]

    @pl.loop(0, tps)
    def _(i):
        at = pl.ds(pl.multiple_of(i * cols, 128), cols)
        total = resid_ref[:, at].astype(F32)
        prod = jnp.dot(mixed[0], proj_all[i, pl.ds(0, lanes), :], preferred_element_type=F32)
        for u in range(1, tps):
            prod += jnp.dot(mixed[u], proj_all[i, pl.ds(u * lanes, lanes), :], preferred_element_type=F32)
        summed[:, at] = total + prod

    block = 64

    @pl.loop(0, tokens // block)
    def _(b):
        at = pl.ds(pl.multiple_of(b * block, block), block)
        x = summed[at, :]
        mean = jnp.mean(x, axis=-1, keepdims=True)
        msq = jnp.mean(x * x, axis=-1, keepdims=True)
        normed[at, :] = ((x - mean) * lax.rsqrt(msq - mean * mean + 1e-05) * gain_ref[...]).astype(BF16)

    gate_up(s, True)
    for k in range(2, n):
        relay(k)
        gate_up_from(k - 1)
    gate_up_from(n - 1)

    edge[0] = gate[pl.ds(PAD, EDGE), :].astype(BF16)
    edge[1] = gate[pl.ds(PAD + tokens - EDGE, EDGE), :].astype(BF16)

    def edge_copy(to_left):
        if to_left:
            return remote(edge.at[0], halo.at[1], edge_send.at[0], edge_recv.at[1], {"sp": s - 1})
        return remote(edge.at[1], halo.at[0], edge_send.at[1], edge_recv.at[0], {"sp": s + 1})

    @pl.when(has_left)
    def _():
        edge_copy(True).start()

    @pl.when(has_right)
    def _():
        edge_copy(False).start()

    strip = 128

    @pl.loop(0, hidden // strip)
    def _(i):
        at = pl.ds(pl.multiple_of(i * strip, strip), strip)
        gate[pl.ds(PAD, tokens), at] = gate[pl.ds(PAD, tokens), at].astype(BF16).astype(F32)

    gate[PAD - 1:PAD, :] = jnp.zeros((1, hidden), F32)
    gate[PAD + tokens:PAD + tokens + 1, :] = jnp.zeros((1, hidden), F32)

    @pl.when(has_left)
    def _():
        edge_copy(False).wait_recv()
        gate[PAD - 1:PAD, :] = halo[0].astype(F32)[EDGE - 1:EDGE, :]

    @pl.when(has_right)
    def _():
        edge_copy(True).wait_recv()
        gate[PAD + tokens:PAD + tokens + 1, :] = halo[1].astype(F32)[0:1, :]

    @pl.loop(0, hidden // strip)
    def _(i):
        at = pl.ds(pl.multiple_of(i * strip, strip), strip)
        conv = cb_ref[:, at]
        for tap in range(CONV):
            conv = conv + gate[pl.ds(PAD - CONV // 2 + tap, tokens), at] * cw_ref[tap:tap + 1, at]
        silu = conv / (1.0 + jnp.exp(-conv))
        act[:, at] = (silu * up[:, at].astype(BF16).astype(F32)).astype(BF16)

    def term_copy(p):
        return remote(terms.at[p], parts.at[t], term_send.at[p], term_recv.at[t], {"tp": p})

    def down(p, first):
        @pl.loop(0, cols // 256)
        def _(i):
            at = pl.ds(pl.multiple_of(i * 256, 256), 256)
            w = wd_ref[:, at] if first else wd_all[p, :, at]
            terms[p, :, at] = jnp.dot(act[...], w, preferred_element_type=F32).astype(BF16)

        @pl.when(p != t)
        def _():
            term_copy(p).start()

    down(s, True)
    for k in range(1, n):
        def do(p):
            arrived(2, p)
            down(p, False)
        pieces(k, do)

    out = normed[:, pl.ds(pl.multiple_of(t * cols, 128), cols)].astype(F32) + terms[t].astype(F32)
    for j in range(1, tps):
        u = lax.rem(t + j, tps)
        remote(terms.at[u], parts.at[u], term_send.at[u], term_recv.at[u], {"tp": u}).wait_recv()
    for j in range(1, tps):
        out = out + parts[lax.rem(t + j, tps)].astype(F32)
    out_ref[...] = out.astype(BF16)

    @pl.when(has_left)
    def _():
        for i in range(2):
            halo_copy(i, True).wait_send()
        edge_copy(True).wait_send()

    @pl.when(has_right)
    def _():
        for i in range(2):
            halo_copy(i, False).wait_send()
        edge_copy(False).wait_send()

    for j in range(1, tps):
        proj_copy(j).wait_send()
        mix_copy(j).wait_send()
        term_copy(lax.rem(t + j, tps)).wait_send()
    for m in range(3):
        for c in range(CHUNKS):
            for able, side in sides:
                @pl.when(able)
                def _(m=m, c=c, side=side):
                    hop(m, s, c, side, True).wait_send()
            for k in range(1, n):
                for side in range(2):
                    p = s - k if side == 0 else s + k
                    here = p >= 0 if side == 0 else p < n

                    @pl.when(here)
                    def _(m=m, c=c, side=side, p=p):
                        for j in range(1, groups):
                            cross(m, p, c, j).wait_send()
                        if k < n - 1:
                            @pl.when(sides[side][0])
                            def _():
                                hop(m, p, c, side, False).wait_send()


def kernel_shards(
    sizes, queries, keys, values, sink, resid, out_proj, norm_gain, w_gate, w_up, conv_w, conv_b, w_down
):
    groups, n, tps = sizes
    tokens, width = resid.shape
    cols = out_proj.shape[1]
    depth, hidden = w_gate.shape
    vmem = pl.BlockSpec(memory_space=pltpu.VMEM)
    dma = pltpu.SemaphoreType.DMA
    shard_sems = dma((3, n, CHUNKS))
    cross_sems = dma((3, n, CHUNKS, groups))
    return pl.pallas_call(
        functools.partial(layer_kernel, sizes),
        out_shape=jax.ShapeDtypeStruct((tokens, cols), BF16),
        in_specs=[vmem] * 3 + [pl.BlockSpec(memory_space=pltpu.SMEM)] + [vmem] * 8,
        out_specs=vmem,
        scratch_shapes=[
            pltpu.VMEM((2, tokens + 2 * WINDOW, HD), BF16),
            pltpu.VMEM((tps,) + out_proj.shape, BF16),
            pltpu.VMEM((tps,) + queries.shape, BF16),
            pltpu.VMEM((tokens, width), F32),
            pltpu.VMEM((tokens, width), BF16),
            pltpu.VMEM((n,) + w_gate.shape, BF16),
            pltpu.VMEM((n,) + w_up.shape, BF16),
            pltpu.VMEM((n,) + w_down.shape, BF16),
            pltpu.VMEM((tokens + 2 * PAD, hidden), F32),
            pltpu.VMEM((tokens, hidden), F32),
            pltpu.VMEM((2, EDGE, hidden), BF16),
            pltpu.VMEM((2, EDGE, hidden), BF16),
            pltpu.VMEM((tokens, hidden), BF16),
            pltpu.VMEM((tps, tokens, cols), BF16),
            pltpu.VMEM((tps, tokens, cols), BF16),
            dma((2, 2)), dma((2, 2)),
            shard_sems, shard_sems, shard_sems, cross_sems, cross_sems,
            dma((tps,)), dma((tps,)), dma((tps,)), dma((tps,)),
            dma((2,)), dma((2,)), dma((tps,)), dma((tps,)),
        ],
        compiler_params=pltpu.CompilerParams(
            collective_id=0, has_side_effects=True, vmem_limit_bytes=64 * 1000 * 1000
        ),
    )(queries, keys, values, sink, resid, out_proj, norm_gain[None], w_gate, w_up, conv_w, conv_b[None], w_down)


def fits_kernel(sizes, args):
    groups, n, tps = sizes
    queries, resid, out_proj, w_gate, w_down = args[0], args[4], args[5], args[7], args[11]
    part = groups * CHUNKS * EDGE
    weights = 3 * 2 * n * w_gate.shape[0] * w_gate.shape[1]
    return (
        n == tps
        and n > 1
        and groups > 1
        and w_down.shape[1] == out_proj.shape[1]
        and w_gate.shape[0] % max(part, 128) == 0
        and w_down.shape[0] % part == 0
        and w_down.shape[1] % 256 == 0
        and w_gate.shape[1] % out_proj.shape[1] == 0
        and resid.shape[0] % WINDOW == 0
        and weights <= 20 * 2 ** 20
    )


def run_shards(sizes, *args):
    if fits_kernel(sizes, args):
        return kernel_shards(sizes, *args)
    return shards(*args)


def solution(mesh):
    sizes = tuple(mesh.shape[axis] for axis in ("grp", "sp", "tp"))
    return jax.shard_map(
        functools.partial(run_shards, sizes),
        mesh=mesh,
        in_specs=(
            P(("grp", "sp"), "tp"),
            P(("grp", "sp"), None),
            P(("grp", "sp"), None),
            P("tp"),
            P(("grp", "sp"), None),
            P(None, "tp"),
            P(),
            P("sp", "tp"),
            P("sp", "tp"),
            P(None, "tp"),
            P("tp"),
            P("tp", "sp"),
        ),
        out_specs=P(("grp", "sp"), "tp"),
        check_vma=False,
    )
```

```python
import functools

import jax
import jax.numpy as jnp
from jax import lax
from jax.experimental import pallas as pl
from jax.experimental.pallas import tpu as pltpu
from jax.sharding import PartitionSpec as P

H = 8
KVH = 2
HD = 128
WINDOW = 128
CONV = 3


def with_halo(cells, sides, width):
    for axis, dim in sides:
        count = lax.axis_size(axis)
        ends = count - 1
        head = lax.slice_in_dim(cells, 0, width, axis=dim)
        tail = lax.slice_in_dim(cells, cells.shape[dim] - width, cells.shape[dim], axis=dim)
        cells = jnp.concatenate(
            [
                lax.ppermute(tail, axis, [(i, (i + 1) % count) for i in range(ends)]),
                cells,
                lax.ppermute(head, axis, [((i + 1) % count, i) for i in range(ends)]),
            ],
            axis=dim,
        )
    return cells


def shards(
    queries, keys, values, sink, resid, out_proj, norm_gain, w_gate, w_up, conv_w, conv_b, w_down
):
    tokens = queries.shape[0]
    width = resid.shape[1]
    heads_here = sink.shape[0]
    group = H // KVH
    scale = HD ** (-0.5)
    first_head = lax.axis_index("tp") * heads_here
    kv_head = first_head // group
    own_keys = lax.dynamic_slice_in_dim(keys, kv_head * HD, HD, 1)
    own_values = lax.dynamic_slice_in_dim(values, kv_head * HD, HD, 1)
    extended = with_halo(jnp.stack([own_keys, own_values]), (("sp", 1),), WINDOW)
    ext_keys = extended[0]
    ext_values = extended[1]
    span = tokens + 2 * WINDOW
    q_heads = queries.reshape(tokens, heads_here, HD)
    scores = (
        jnp.einsum("qhd,kd->hqk", q_heads, ext_keys, preferred_element_type=jnp.float32) * scale
    )
    offset = lax.axis_index("sp") * tokens
    q_pos = offset + jnp.arange(tokens, dtype=jnp.int32)[:, None]
    k_pos = offset - WINDOW + jnp.arange(span, dtype=jnp.int32)[None, :]
    seq_total = tokens * lax.axis_size("sp")
    valid = (jnp.abs(q_pos - k_pos) <= WINDOW) & (k_pos >= 0) & (k_pos < seq_total)
    scores = jnp.where(valid[None], scores, jnp.float32(-1e30))
    sink_col = sink[:, None]
    top = jnp.maximum(jnp.max(scores, axis=-1), sink_col)
    expo = jnp.exp(scores - top[..., None])
    total = jnp.sum(expo, axis=-1) + jnp.exp(sink_col - top)
    weights = (expo / total[..., None]).astype(jnp.bfloat16)
    heads_out = jnp.einsum("hqk,kd->qhd", weights, ext_values, preferred_element_type=jnp.float32)
    heads_out = heads_out.astype(jnp.bfloat16).reshape(tokens, heads_here * HD)
    all_heads = lax.all_gather(heads_out, "tp", axis=1, tiled=True)
    cols = width // lax.axis_size("tp")
    col_start = lax.axis_index("tp") * cols
    full_proj = lax.all_gather(out_proj, "tp", axis=1, tiled=True)
    summed = resid.astype(jnp.float32) + jnp.dot(
        all_heads, full_proj, preferred_element_type=jnp.float32
    )
    mean = jnp.mean(summed, axis=-1, keepdims=True)
    msq = jnp.mean(summed * summed, axis=-1, keepdims=True)
    normed_full = ((summed - mean) * lax.rsqrt(msq - mean * mean + 1e-05) * norm_gain).astype(
        jnp.bfloat16
    )
    normed_own = lax.dynamic_slice_in_dim(normed_full, col_start, cols, 1)
    gate_acc = jnp.dot(
        normed_full,
        lax.all_gather(w_gate, "sp", axis=0, tiled=True),
        preferred_element_type=jnp.float32,
    )
    up_acc = jnp.dot(
        normed_full,
        lax.all_gather(w_up, "sp", axis=0, tiled=True),
        preferred_element_type=jnp.float32,
    )
    gate_pre = gate_acc.astype(jnp.bfloat16)
    up_part = up_acc.astype(jnp.bfloat16)
    padded = with_halo(gate_pre, (("sp", 0),), CONV // 2)
    conv = conv_b
    for tap in range(CONV):
        conv = conv + padded[tap : tap + tokens].astype(jnp.float32) * conv_w[tap]
    act = (jax.nn.silu(conv) * up_part.astype(jnp.float32)).astype(jnp.bfloat16)
    terms = jnp.dot(
        act, lax.all_gather(w_down, "sp", axis=1, tiled=True), preferred_element_type=jnp.float32
    )
    ffn_own = lax.psum_scatter(
        terms.astype(jnp.bfloat16), "tp", scatter_dimension=1, tiled=True
    ).astype(jnp.float32)
    return (normed_own.astype(jnp.float32) + ffn_own).astype(jnp.bfloat16)


CHUNKS = 2
CROSSED = 1
PAD = 8
EDGE = 16
BF16 = jnp.bfloat16
F32 = jnp.float32


def layer_kernel(
    sizes,
    q_ref, k_ref, v_ref, sink_ref, resid_ref, proj_ref, gain_ref, wg_ref, wu_ref, cw_ref, cb_ref, wd_ref,
    out_ref,
    kv_ext, proj_all, mixed, summed, normed, wg_all, wu_all, wd_all, gate, up, edge, halo, act, terms, parts,
    ret_out, ret_in,
    halo_send, halo_recv, z_recv, z_send, y_recv, y_send,
    proj_send, proj_recv, mix_send, mix_recv, norm_send, norm_recv, edge_send, edge_recv,
    term_send, term_recv, ret_send, ret_recv,
):
    groups, n, tps = sizes
    g = lax.axis_index("grp")
    s = lax.axis_index("sp")
    t = lax.axis_index("tp")
    tokens, width = resid_ref.shape
    heads_here = sink_ref.shape[0]
    cols = proj_ref.shape[1]
    depth = wg_ref.shape[0]
    hidden = wg_ref.shape[1]
    rows2 = 2 * tokens
    has_left, has_right = s > 0, s < n - 1
    inner = has_left & has_right
    outer = jnp.logical_not(inner)
    low = s < n // 2
    inward = 1 - 2 * (s // (n // 2))
    base = pl.multiple_of(lax.rem(s, 2) * tokens, tokens)
    other_base = pl.multiple_of((1 - lax.rem(s, 2)) * tokens, tokens)
    core_peer = t + 1 - 2 * lax.rem(t, 2)
    chip_peer = lax.rem(t + 2, tps)
    own = (wg_ref, wu_ref, wd_ref)
    full = (wg_all, wu_all, wd_all)

    def remote(src, dst, send, recv, to):
        return pltpu.make_async_remote_copy(
            src_ref=src, dst_ref=dst, send_sem=send, recv_sem=recv,
            device_id=to, device_id_type=pl.DeviceIdType.MESH,
        )

    barrier = pltpu.get_barrier_semaphore()

    def greet(to):
        pl.semaphore_signal(barrier, inc=1, device_id=to, device_id_type=pl.DeviceIdType.MESH)

    @pl.when(has_left)
    def _():
        greet({"sp": s - 1})

    @pl.when(has_right)
    def _():
        greet({"sp": s + 1})

    for j in range(1, groups):
        greet({"grp": lax.rem(g + j, groups)})
    for j in range(1, tps):
        greet({"tp": lax.rem(t + j, tps)})
    along = jnp.minimum(s, 1) + jnp.minimum(n - 1 - s, 1)
    pl.semaphore_wait(barrier, along + groups - 1 + tps - 1)

    kv_head = (t * heads_here) // (H // KVH)
    kv_cols = pl.ds(pl.multiple_of(kv_head * HD, HD), HD)

    def halo_copy(i, to_left):
        ref = (k_ref, v_ref)[i]
        if to_left:
            return remote(ref.at[pl.ds(0, WINDOW), kv_cols], kv_ext.at[i, pl.ds(WINDOW + tokens, WINDOW)],
                          halo_send.at[i, 0], halo_recv.at[i, 0], {"sp": s - 1})
        return remote(ref.at[pl.ds(tokens - WINDOW, WINDOW), kv_cols], kv_ext.at[i, pl.ds(0, WINDOW)],
                      halo_send.at[i, 1], halo_recv.at[i, 1], {"sp": s + 1})

    def rows_of(m, part, c):
        step = own[m].shape[0] // (groups * CHUNKS)
        return pl.ds(pl.multiple_of((part * CHUNKS + c) * step, EDGE), step)

    def hop(m, src_slot, dst_slot, j, c):
        part = lax.rem(g + j, groups)
        rows = rows_of(m, part, c)
        src = own[m].at[rows] if src_slot is None else full[m].at[src_slot, rows]
        return remote(src, full[m].at[dst_slot, rows], z_send.at[m, 0 if src_slot is None else 1, j, c],
                      z_recv.at[m, dst_slot, j, c], {"sp": s + inward})

    def cross(m, slot, c, j):
        rows = rows_of(m, g, c)
        return remote(full[m].at[slot, rows], full[m].at[slot, rows], y_send.at[m, slot, c, j],
                      y_recv.at[m, slot, c, j], {"grp": lax.rem(g + j, groups)})

    def cross_arrival(m, slot, c, j):
        rows = rows_of(m, lax.rem(g + groups - j, groups), c)
        return remote(full[m].at[slot, rows], full[m].at[slot, rows], y_send.at[m, slot, c, j],
                      y_recv.at[m, slot, c, j], {"grp": lax.rem(g + j, groups)})

    pieces = [(m, c) for m in range(3) for c in range(CHUNKS)]
    crossed = pieces[:CROSSED]
    direct = [(m, c, j) for m, c in pieces[CROSSED:] for j in range(1, groups)]

    def spread(src, ref, send, recv, step):
        origin = (t, t, chip_peer)[step]
        return remote(src if step < 2 else ref.at[origin], ref.at[origin], send.at[step], recv.at[step],
                      {"tp": (core_peer, chip_peer, core_peer)[step]})

    def spread_arrival(src, ref, send, recv, step):
        origin = (core_peer, chip_peer, lax.rem(core_peer + 2, tps))[step]
        return remote(src, ref.at[origin], send.at[step], recv.at[step],
                      {"tp": (core_peer, chip_peer, core_peer)[step]})

    proj_args = (proj_ref, proj_all, proj_send, proj_recv)
    mix_args = (mixed.at[t], mixed, mix_send, mix_recv)

    @pl.when(has_left)
    def _():
        for i in range(2):
            halo_copy(i, True).start()

    @pl.when(has_right)
    def _():
        for i in range(2):
            halo_copy(i, False).start()

    @pl.when(outer)
    def _():
        for m, c in pieces:
            hop(m, None, 0, 0, c).start()

    @pl.when(inner)
    def _():
        for m, c in pieces:
            hop(m, None, 1, 0, c).start()

    for step in (1, 0):
        spread(*proj_args, step).start()

    for i, ref in enumerate((k_ref, v_ref)):
        kv_ext[i, pl.ds(WINDOW, tokens), :] = ref[:, kv_cols]

    @pl.when(jnp.logical_not(has_left))
    def _():
        kv_ext[:, pl.ds(0, WINDOW), :] = jnp.zeros((2, WINDOW, HD), BF16)

    @pl.when(jnp.logical_not(has_right))
    def _():
        kv_ext[:, pl.ds(WINDOW + tokens, WINDOW), :] = jnp.zeros((2, WINDOW, HD), BF16)

    @pl.when(has_right)
    def _():
        for i in range(2):
            halo_copy(i, True).wait_recv()

    @pl.when(has_left)
    def _():
        for i in range(2):
            halo_copy(i, False).wait_recv()

    span = 3 * WINDOW
    seq_total = tokens * n

    @pl.loop(0, tokens // WINDOW)
    def _(b):
        start = pl.multiple_of(b * WINDOW, WINDOW)
        row = lax.broadcasted_iota(jnp.int32, (WINDOW, span), 0)
        col = lax.broadcasted_iota(jnp.int32, (WINDOW, span), 1)
        k_pos = s * tokens + start - WINDOW + col
        valid = (jnp.abs(row + WINDOW - col) <= WINDOW) & (k_pos >= 0) & (k_pos < seq_total)
        kb = kv_ext[0, pl.ds(start, span), :]
        vb = kv_ext[1, pl.ds(start, span), :]
        for h in range(heads_here):
            qb = q_ref[pl.ds(start, WINDOW), h * HD:(h + 1) * HD]
            sc = lax.dot_general(qb, kb, (((1,), (1,)), ((), ())), preferred_element_type=F32) * (HD ** -0.5)
            sc = jnp.where(valid, sc, F32(-1e30))
            sink = sink_ref[h]
            top = jnp.maximum(jnp.max(sc, axis=-1, keepdims=True), sink)
            expo = jnp.exp(sc - top)
            total = jnp.sum(expo, axis=-1, keepdims=True) + jnp.exp(sink - top)
            weights = (expo / total).astype(BF16)
            o = jnp.dot(weights, vb, preferred_element_type=F32)
            mixed[t, pl.ds(start, WINDOW), h * HD:(h + 1) * HD] = o.astype(BF16)

    proj_all[t] = proj_ref[...]
    for step in (1, 0):
        spread(*mix_args, step).start()

    def relay_near(m):
        for c in range(CHUNKS):
            hop(m, None, 0, 0, c).wait_recv()
            hop(m, 0, 2, 0, c).start()
            if (m, c) in crossed:
                for j in range(1, groups):
                    cross(m, 0, c, j).start()
            hop(m, None, 1, 0, c).wait_recv()
            for j in range(1, groups):
                cross(m, 1, c, j).start()

    def relay_far(m):
        for c in range(CHUNKS):
            hop(m, 0, 2, 0, c).wait_recv()
            for j in range(1, groups):
                cross(m, 2, c, j).start()

    @pl.when(inner)
    def _():
        relay_near(0)

    for args in (proj_args, mix_args):
        spread_arrival(*args, 1).wait_recv()
        spread(*args, 2).start()
    for args in (proj_args, mix_args):
        for step in (0, 2):
            spread_arrival(*args, step).wait_recv()
    lanes = mixed.shape[2]
    block = summed.shape[0]
    strip = 64

    @pl.loop(0, tokens // block)
    def _(b):
        rows = pl.ds(pl.multiple_of(b * block, block), block)

        @pl.loop(0, tps)
        def _(i):
            at = pl.ds(pl.multiple_of(i * cols, 128), cols)
            prod = jnp.dot(mixed[0, rows, :], proj_all[i, pl.ds(0, lanes), :], preferred_element_type=F32)
            for u in range(1, tps):
                prod += jnp.dot(mixed[u, rows, :], proj_all[i, pl.ds(u * lanes, lanes), :],
                                preferred_element_type=F32)
            summed[:, at] = resid_ref[rows, at].astype(F32) + prod

        @pl.loop(0, block // strip)
        def _(i):
            at = pl.multiple_of(i * strip, strip)
            x = summed[pl.ds(at, strip), :]
            mean = jnp.mean(x, axis=-1, keepdims=True)
            msq = jnp.mean(x * x, axis=-1, keepdims=True)
            normed[pl.ds(pl.multiple_of(base + b * block + at, strip), strip), :] = (
                (x - mean) * lax.rsqrt(msq - mean * mean + 1e-05) * gain_ref[...]
            ).astype(BF16)

    half = width // 2
    my_half = pl.ds(pl.multiple_of(lax.rem(t, 2) * half, half), half)
    peer_half = pl.ds(pl.multiple_of((1 - lax.rem(t, 2)) * half, half), half)

    def norm_in():
        part = normed.at[pl.ds(base, tokens), my_half]
        return remote(part, part, norm_send.at[0], norm_recv.at[0], {"sp": s + inward})

    def norm_in_arrival():
        part = normed.at[pl.ds(other_base, tokens), my_half]
        return remote(part, part, norm_send.at[0], norm_recv.at[0], {"sp": s + inward})

    def norm_over(of_peer):
        part = normed.at[pl.ds(other_base, tokens), peer_half if of_peer else my_half]
        return remote(part, part, norm_send.at[1], norm_recv.at[1], {"tp": core_peer})

    def ret_copy():
        return remote(ret_out, ret_in, ret_send.at[0], ret_recv.at[0], {"sp": s - inward})

    def edge_copy():
        return remote(edge, halo, edge_send.at[0], edge_recv.at[0], {"sp": s + inward})

    def term_copy(p, own_rows):
        rows = pl.ds(base if own_rows else other_base, tokens)
        i = int(own_rows)
        return remote(terms.at[p, rows], parts.at[t, rows], term_send.at[p, i], term_recv.at[t, i], {"tp": p})

    def term_arrival(u, own_rows):
        rows = pl.ds(base if own_rows else other_base, tokens)
        i = int(own_rows)
        return remote(terms.at[u, rows], parts.at[u, rows], term_send.at[u, i], term_recv.at[u, i], {"tp": u})

    tile = 256
    my_cols = pl.ds(pl.multiple_of(t * cols, 128), cols)

    def arrived(m, slot):
        for c in range(CHUNKS):
            for j in range(1, groups):
                if slot == 0 and (m, c) not in crossed:
                    hop(m, None, 0, j, c).wait_recv()
                else:
                    cross_arrival(m, slot, c, j).wait_recv()

    def gate_up(slot):
        if slot is not None:
            arrived(0, slot)
            arrived(1, slot)
        p = s + {None: 0, 0: -1, 1: 1, 2: 2}[slot] * inward

        @pl.loop(0, hidden // tile)
        def _(i):
            at = pl.ds(pl.multiple_of(i * tile, 128), tile)
            x = normed[:, pl.ds(pl.multiple_of(p * depth, 128), depth)]
            wa = wg_ref[:, at] if slot is None else wg_all[slot, :, at]
            ga = jnp.dot(x, wa, preferred_element_type=F32)
            if slot is None:
                gate[pl.ds(PAD, rows2), at] = ga
            else:
                gate[pl.ds(PAD, rows2), at] += ga
            wb = wu_ref[:, at] if slot is None else wu_all[slot, :, at]
            ub = jnp.dot(x, wb, preferred_element_type=F32)
            if slot is None:
                up[:, at] = ub
            else:
                up[:, at] += ub

    def down(slot):
        if slot is not None:
            arrived(2, slot)
        p = s + {None: 0, 0: -1, 1: 1, 2: 2}[slot] * inward
        for own_rows in (False, True):
            rows = pl.ds(base if own_rows else other_base, tokens)

            @pl.loop(0, cols // tile)
            def _(i):
                at = pl.ds(pl.multiple_of(i * tile, 128), tile)
                w = wd_ref[:, at] if slot is None else wd_all[slot, :, at]
                terms[p, rows, at] = jnp.dot(act[rows, :], w, preferred_element_type=F32).astype(BF16)

            @pl.when(p != t)
            def _():
                term_copy(p, own_rows).start()

    def finish(own_rows):
        rows = pl.ds(base if own_rows else other_base, tokens)
        out = normed[rows, my_cols].astype(F32) + terms[t, rows, :].astype(F32)
        for j in range(1, tps):
            u = lax.rem(t + j, tps)
            term_arrival(u, own_rows).wait_recv()
            out = out + parts[u, rows, :].astype(F32)
        return out.astype(BF16)

    @pl.when(outer)
    def _():
        norm_in().start()
        for m, c, j in direct:
            hop(m, None, 0, j, c).start()
        ret_copy().wait_recv()
        out_ref[...] = ret_in[...]
        norm_in().wait_send()
        for m, c, j in direct:
            hop(m, None, 0, j, c).wait_send()
        for m, c in pieces:
            hop(m, None, 0, 0, c).wait_send()

    @pl.when(inner)
    def _():
        relay_near(1)
        relay_near(2)
        relay_far(0)
        norm_in_arrival().wait_recv()
        norm_over(False).start()
        relay_far(1)
        norm_over(True).wait_recv()
        gate_up(None)
        gate_up(1)
        relay_far(2)
        gate_up(0)
        gate_up(2)

        at_edge = pl.multiple_of(PAD + (1 - s // (n // 2)) * (rows2 - EDGE), PAD)
        edge[...] = gate[pl.ds(at_edge, EDGE), :].astype(BF16)
        edge_copy().start()
        gate[PAD - 1:PAD, :] = jnp.zeros((1, hidden), F32)
        gate[PAD + rows2:PAD + rows2 + 1, :] = jnp.zeros((1, hidden), F32)
        edge_copy().wait_recv()

        @pl.when(low)
        def _():
            gate[PAD + rows2:PAD + rows2 + 1, :] = halo[...].astype(F32)[0:1, :]

        @pl.when(jnp.logical_not(low))
        def _():
            gate[PAD - 1:PAD, :] = halo[...].astype(F32)[EDGE - 1:EDGE, :]

        @pl.loop(0, hidden // 128)
        def _(i):
            at = pl.ds(pl.multiple_of(i * 128, 128), 128)
            gate[pl.ds(PAD, rows2), at] = gate[pl.ds(PAD, rows2), at].astype(BF16).astype(F32)
            conv = cb_ref[:, at]
            for tap in range(CONV):
                conv = conv + gate[pl.ds(PAD - CONV // 2 + tap, rows2), at] * cw_ref[tap:tap + 1, at]
            silu = conv / (1.0 + jnp.exp(-conv))
            act[:, at] = (silu * up[:, at].astype(BF16).astype(F32)).astype(BF16)

        down(None)
        down(1)
        down(2)
        down(0)
        ret_out[...] = finish(False)
        ret_copy().start()
        out_ref[...] = finish(True)

        ret_copy().wait_send()
        edge_copy().wait_send()
        norm_over(False).wait_send()
        for j in range(1, tps):
            for own_rows in (False, True):
                term_copy(lax.rem(t + j, tps), own_rows).wait_send()
        for m, c in pieces:
            hop(m, None, 1, 0, c).wait_send()
            hop(m, 0, 2, 0, c).wait_send()
            for j in range(1, groups):
                if (m, c) in crossed:
                    cross(m, 0, c, j).wait_send()
                cross(m, 1, c, j).wait_send()
                cross(m, 2, c, j).wait_send()

    @pl.when(has_left)
    def _():
        for i in range(2):
            halo_copy(i, True).wait_send()

    @pl.when(has_right)
    def _():
        for i in range(2):
            halo_copy(i, False).wait_send()

    for step in range(3):
        spread(*proj_args, step).wait_send()
        spread(*mix_args, step).wait_send()


def kernel_shards(
    sizes, queries, keys, values, sink, resid, out_proj, norm_gain, w_gate, w_up, conv_w, conv_b, w_down
):
    groups, n, tps = sizes
    tokens, width = resid.shape
    cols = out_proj.shape[1]
    depth, hidden = w_gate.shape
    vmem = pl.BlockSpec(memory_space=pltpu.VMEM)
    dma = pltpu.SemaphoreType.DMA
    cross_sems = dma((3, 3, CHUNKS, groups))
    return pl.pallas_call(
        functools.partial(layer_kernel, sizes),
        out_shape=jax.ShapeDtypeStruct((tokens, cols), BF16),
        in_specs=[vmem] * 3 + [pl.BlockSpec(memory_space=pltpu.SMEM)] + [vmem] * 8,
        out_specs=vmem,
        scratch_shapes=[
            pltpu.VMEM((2, tokens + 2 * WINDOW, HD), BF16),
            pltpu.VMEM((tps,) + out_proj.shape, BF16),
            pltpu.VMEM((tps,) + queries.shape, BF16),
            pltpu.VMEM((tokens // 2, width), F32),
            pltpu.VMEM((2 * tokens, width), BF16),
            pltpu.VMEM((n - 1,) + w_gate.shape, BF16),
            pltpu.VMEM((n - 1,) + w_up.shape, BF16),
            pltpu.VMEM((n - 1,) + w_down.shape, BF16),
            pltpu.VMEM((2 * tokens + 2 * PAD, hidden), F32),
            pltpu.VMEM((2 * tokens, hidden), F32),
            pltpu.VMEM((EDGE, hidden), BF16),
            pltpu.VMEM((EDGE, hidden), BF16),
            pltpu.VMEM((2 * tokens, hidden), BF16),
            pltpu.VMEM((tps, 2 * tokens, cols), BF16),
            pltpu.VMEM((tps, 2 * tokens, cols), BF16),
            pltpu.VMEM((tokens, cols), BF16),
            pltpu.VMEM((tokens, cols), BF16),
            dma((2, 2)), dma((2, 2)),
            dma((3, 3, groups, CHUNKS)), dma((3, 2, groups, CHUNKS)),
            cross_sems, cross_sems,
            dma((3,)), dma((3,)), dma((3,)), dma((3,)), dma((2,)), dma((2,)), dma((1,)), dma((1,)),
            dma((tps, 2)), dma((tps, 2)), dma((1,)), dma((1,)),
        ],
        compiler_params=pltpu.CompilerParams(
            collective_id=0, has_side_effects=True, vmem_limit_bytes=67043328
        ),
    )(queries, keys, values, sink, resid, out_proj, norm_gain[None], w_gate, w_up, conv_w, conv_b[None], w_down)


def fits_kernel(sizes, args):
    groups, n, tps = sizes
    queries, resid, out_proj, w_gate, w_down = args[0], args[4], args[5], args[7], args[11]
    part = groups * CHUNKS * EDGE
    weights = 3 * 2 * n * w_gate.shape[0] * w_gate.shape[1]
    return (
        n == 4
        and tps == 4
        and groups > 1
        and w_down.shape[1] == out_proj.shape[1]
        and w_gate.shape[0] % max(part, 128) == 0
        and w_down.shape[0] % part == 0
        and w_down.shape[1] % 256 == 0
        and w_gate.shape[1] % out_proj.shape[1] == 0
        and resid.shape[0] % (4 * WINDOW) == 0
        and weights <= 20 * 2 ** 20
    )


def run_shards(sizes, *args):
    if fits_kernel(sizes, args):
        return kernel_shards(sizes, *args)
    return shards(*args)


def solution(mesh):
    sizes = tuple(mesh.shape[axis] for axis in ("grp", "sp", "tp"))
    return jax.shard_map(
        functools.partial(run_shards, sizes),
        mesh=mesh,
        in_specs=(
            P(("grp", "sp"), "tp"),
            P(("grp", "sp"), None),
            P(("grp", "sp"), None),
            P("tp"),
            P(("grp", "sp"), None),
            P(None, "tp"),
            P(),
            P("sp", "tp"),
            P("sp", "tp"),
            P(None, "tp"),
            P("tp"),
            P("tp", "sp"),
        ),
        out_specs=P(("grp", "sp"), "tp"),
        check_vma=False,
    )
```

```python
import functools

import jax
import jax.numpy as jnp
from jax import lax
from jax.experimental import pallas as pl
from jax.experimental.pallas import tpu as pltpu
from jax.sharding import PartitionSpec as P

H = 8
KVH = 2
HD = 128
WINDOW = 128
CONV = 3


def with_halo(cells, sides, width):
    for axis, dim in sides:
        count = lax.axis_size(axis)
        ends = count - 1
        head = lax.slice_in_dim(cells, 0, width, axis=dim)
        tail = lax.slice_in_dim(cells, cells.shape[dim] - width, cells.shape[dim], axis=dim)
        cells = jnp.concatenate(
            [
                lax.ppermute(tail, axis, [(i, (i + 1) % count) for i in range(ends)]),
                cells,
                lax.ppermute(head, axis, [((i + 1) % count, i) for i in range(ends)]),
            ],
            axis=dim,
        )
    return cells


def shards(
    queries, keys, values, sink, resid, out_proj, norm_gain, w_gate, w_up, conv_w, conv_b, w_down
):
    tokens = queries.shape[0]
    width = resid.shape[1]
    heads_here = sink.shape[0]
    group = H // KVH
    scale = HD ** (-0.5)
    first_head = lax.axis_index("tp") * heads_here
    kv_head = first_head // group
    own_keys = lax.dynamic_slice_in_dim(keys, kv_head * HD, HD, 1)
    own_values = lax.dynamic_slice_in_dim(values, kv_head * HD, HD, 1)
    extended = with_halo(jnp.stack([own_keys, own_values]), (("sp", 1),), WINDOW)
    ext_keys = extended[0]
    ext_values = extended[1]
    span = tokens + 2 * WINDOW
    q_heads = queries.reshape(tokens, heads_here, HD)
    scores = (
        jnp.einsum("qhd,kd->hqk", q_heads, ext_keys, preferred_element_type=jnp.float32) * scale
    )
    offset = lax.axis_index("sp") * tokens
    q_pos = offset + jnp.arange(tokens, dtype=jnp.int32)[:, None]
    k_pos = offset - WINDOW + jnp.arange(span, dtype=jnp.int32)[None, :]
    seq_total = tokens * lax.axis_size("sp")
    valid = (jnp.abs(q_pos - k_pos) <= WINDOW) & (k_pos >= 0) & (k_pos < seq_total)
    scores = jnp.where(valid[None], scores, jnp.float32(-1e30))
    sink_col = sink[:, None]
    top = jnp.maximum(jnp.max(scores, axis=-1), sink_col)
    expo = jnp.exp(scores - top[..., None])
    total = jnp.sum(expo, axis=-1) + jnp.exp(sink_col - top)
    weights = (expo / total[..., None]).astype(jnp.bfloat16)
    heads_out = jnp.einsum("hqk,kd->qhd", weights, ext_values, preferred_element_type=jnp.float32)
    heads_out = heads_out.astype(jnp.bfloat16).reshape(tokens, heads_here * HD)
    all_heads = lax.all_gather(heads_out, "tp", axis=1, tiled=True)
    cols = width // lax.axis_size("tp")
    col_start = lax.axis_index("tp") * cols
    full_proj = lax.all_gather(out_proj, "tp", axis=1, tiled=True)
    summed = resid.astype(jnp.float32) + jnp.dot(
        all_heads, full_proj, preferred_element_type=jnp.float32
    )
    mean = jnp.mean(summed, axis=-1, keepdims=True)
    msq = jnp.mean(summed * summed, axis=-1, keepdims=True)
    normed_full = ((summed - mean) * lax.rsqrt(msq - mean * mean + 1e-05) * norm_gain).astype(
        jnp.bfloat16
    )
    normed_own = lax.dynamic_slice_in_dim(normed_full, col_start, cols, 1)
    gate_acc = jnp.dot(
        normed_full,
        lax.all_gather(w_gate, "sp", axis=0, tiled=True),
        preferred_element_type=jnp.float32,
    )
    up_acc = jnp.dot(
        normed_full,
        lax.all_gather(w_up, "sp", axis=0, tiled=True),
        preferred_element_type=jnp.float32,
    )
    gate_pre = gate_acc.astype(jnp.bfloat16)
    up_part = up_acc.astype(jnp.bfloat16)
    padded = with_halo(gate_pre, (("sp", 0),), CONV // 2)
    conv = conv_b
    for tap in range(CONV):
        conv = conv + padded[tap : tap + tokens].astype(jnp.float32) * conv_w[tap]
    act = (jax.nn.silu(conv) * up_part.astype(jnp.float32)).astype(jnp.bfloat16)
    terms = jnp.dot(
        act, lax.all_gather(w_down, "sp", axis=1, tiled=True), preferred_element_type=jnp.float32
    )
    ffn_own = lax.psum_scatter(
        terms.astype(jnp.bfloat16), "tp", scatter_dimension=1, tiled=True
    ).astype(jnp.float32)
    return (normed_own.astype(jnp.float32) + ffn_own).astype(jnp.bfloat16)


CHUNKS = 2
CROSSED = 1
PAD = 8
EDGE = 16
BF16 = jnp.bfloat16
F32 = jnp.float32


def layer_kernel(
    sizes,
    q_ref, k_ref, v_ref, sink_ref, resid_ref, proj_ref, gain_ref, wg_ref, wu_ref, cw_ref, cb_ref, wd_ref,
    out_ref,
    kv_ext, proj_all, mixed, summed, normed, wg_all, wu_all, wd_all, gate, up, edge, halo, act, terms, parts,
    pair_in, ret_out, ret_in,
    halo_send, halo_recv, z_recv, z_send, y_recv, y_send,
    proj_send, proj_recv, mix_send, mix_recv, norm_send, norm_recv, edge_send, edge_recv,
    term_send, term_recv, pair_send, pair_recv, ret_send, ret_recv,
):
    groups, n, tps = sizes
    g = lax.axis_index("grp")
    s = lax.axis_index("sp")
    t = lax.axis_index("tp")
    tokens, width = resid_ref.shape
    heads_here = sink_ref.shape[0]
    cols = proj_ref.shape[1]
    depth = wg_ref.shape[0]
    hidden = wg_ref.shape[1]
    rows2 = 2 * tokens
    has_left, has_right = s > 0, s < n - 1
    inner = has_left & has_right
    outer = jnp.logical_not(inner)
    low = s < n // 2
    inward = 1 - 2 * (s // (n // 2))
    base = pl.multiple_of(lax.rem(s, 2) * tokens, tokens)
    other_base = pl.multiple_of((1 - lax.rem(s, 2)) * tokens, tokens)
    core_peer = t + 1 - 2 * lax.rem(t, 2)
    chip_peer = lax.rem(t + 2, tps)
    own = (wg_ref, wu_ref, wd_ref)
    full = (wg_all, wu_all, wd_all)

    def remote(src, dst, send, recv, to):
        return pltpu.make_async_remote_copy(
            src_ref=src, dst_ref=dst, send_sem=send, recv_sem=recv,
            device_id=to, device_id_type=pl.DeviceIdType.MESH,
        )

    barrier = pltpu.get_barrier_semaphore()

    def greet(to):
        pl.semaphore_signal(barrier, inc=1, device_id=to, device_id_type=pl.DeviceIdType.MESH)

    @pl.when(has_left)
    def _():
        greet({"sp": s - 1})

    @pl.when(has_right)
    def _():
        greet({"sp": s + 1})

    for j in range(1, groups):
        greet({"grp": lax.rem(g + j, groups)})
    for j in range(1, tps):
        greet({"tp": lax.rem(t + j, tps)})
    along = jnp.minimum(s, 1) + jnp.minimum(n - 1 - s, 1)
    pl.semaphore_wait(barrier, along + groups - 1 + tps - 1)

    kv_head = (t * heads_here) // (H // KVH)
    kv_cols = pl.ds(pl.multiple_of(kv_head * HD, HD), HD)

    def halo_copy(i, to_left):
        ref = (k_ref, v_ref)[i]
        if to_left:
            return remote(ref.at[pl.ds(0, WINDOW), kv_cols], kv_ext.at[i, pl.ds(WINDOW + tokens, WINDOW)],
                          halo_send.at[i, 0], halo_recv.at[i, 0], {"sp": s - 1})
        return remote(ref.at[pl.ds(tokens - WINDOW, WINDOW), kv_cols], kv_ext.at[i, pl.ds(0, WINDOW)],
                      halo_send.at[i, 1], halo_recv.at[i, 1], {"sp": s + 1})

    def rows_of(m, part, c):
        step = own[m].shape[0] // (groups * CHUNKS)
        return pl.ds(pl.multiple_of((part * CHUNKS + c) * step, EDGE), step)

    def hop(m, src_slot, dst_slot, j, c):
        part = lax.rem(g + j, groups)
        rows = rows_of(m, part, c)
        src = own[m].at[rows] if src_slot is None else full[m].at[src_slot, rows]
        return remote(src, full[m].at[dst_slot, rows], z_send.at[m, 0 if src_slot is None else 1, j, c],
                      z_recv.at[m, dst_slot, j, c], {"sp": s + inward})

    def cross(m, slot, c, j):
        rows = rows_of(m, g, c)
        return remote(full[m].at[slot, rows], full[m].at[slot, rows], y_send.at[m, slot, c, j],
                      y_recv.at[m, slot, c, j], {"grp": lax.rem(g + j, groups)})

    def cross_arrival(m, slot, c, j):
        rows = rows_of(m, lax.rem(g + groups - j, groups), c)
        return remote(full[m].at[slot, rows], full[m].at[slot, rows], y_send.at[m, slot, c, j],
                      y_recv.at[m, slot, c, j], {"grp": lax.rem(g + j, groups)})

    pieces = [(m, c) for m in range(3) for c in range(CHUNKS)]
    crossed = pieces[:CROSSED]
    direct = [(m, c, j) for m, c in pieces[CROSSED:] for j in range(1, groups)]

    def spread(src, ref, send, recv, step):
        origin = (t, t, chip_peer)[step]
        return remote(src if step < 2 else ref.at[origin], ref.at[origin], send.at[step], recv.at[step],
                      {"tp": (core_peer, chip_peer, core_peer)[step]})

    def spread_arrival(src, ref, send, recv, step):
        origin = (core_peer, chip_peer, lax.rem(core_peer + 2, tps))[step]
        return remote(src, ref.at[origin], send.at[step], recv.at[step],
                      {"tp": (core_peer, chip_peer, core_peer)[step]})

    proj_args = (proj_ref, proj_all, proj_send, proj_recv)
    mix_args = (mixed.at[t], mixed, mix_send, mix_recv)

    @pl.when(has_left)
    def _():
        for i in range(2):
            halo_copy(i, True).start()

    @pl.when(has_right)
    def _():
        for i in range(2):
            halo_copy(i, False).start()

    @pl.when(outer)
    def _():
        for m, c in pieces:
            hop(m, None, 0, 0, c).start()

    @pl.when(inner)
    def _():
        for m, c in pieces:
            hop(m, None, 1, 0, c).start()

    for step in (1, 0):
        spread(*proj_args, step).start()

    for i, ref in enumerate((k_ref, v_ref)):
        kv_ext[i, pl.ds(WINDOW, tokens), :] = ref[:, kv_cols]

    @pl.when(jnp.logical_not(has_left))
    def _():
        kv_ext[:, pl.ds(0, WINDOW), :] = jnp.zeros((2, WINDOW, HD), BF16)

    @pl.when(jnp.logical_not(has_right))
    def _():
        kv_ext[:, pl.ds(WINDOW + tokens, WINDOW), :] = jnp.zeros((2, WINDOW, HD), BF16)

    @pl.when(has_right)
    def _():
        for i in range(2):
            halo_copy(i, True).wait_recv()

    @pl.when(has_left)
    def _():
        for i in range(2):
            halo_copy(i, False).wait_recv()

    span = 3 * WINDOW
    seq_total = tokens * n

    @pl.loop(0, tokens // WINDOW)
    def _(b):
        start = pl.multiple_of(b * WINDOW, WINDOW)
        row = lax.broadcasted_iota(jnp.int32, (WINDOW, span), 0)
        col = lax.broadcasted_iota(jnp.int32, (WINDOW, span), 1)
        k_pos = s * tokens + start - WINDOW + col
        valid = (jnp.abs(row + WINDOW - col) <= WINDOW) & (k_pos >= 0) & (k_pos < seq_total)
        kb = kv_ext[0, pl.ds(start, span), :]
        vb = kv_ext[1, pl.ds(start, span), :]
        for h in range(heads_here):
            qb = q_ref[pl.ds(start, WINDOW), h * HD:(h + 1) * HD]
            sc = lax.dot_general(qb, kb, (((1,), (1,)), ((), ())), preferred_element_type=F32) * (HD ** -0.5)
            sc = jnp.where(valid, sc, F32(-1e30))
            sink = sink_ref[h]
            top = jnp.maximum(jnp.max(sc, axis=-1, keepdims=True), sink)
            expo = jnp.exp(sc - top)
            total = jnp.sum(expo, axis=-1, keepdims=True) + jnp.exp(sink - top)
            weights = (expo / total).astype(BF16)
            o = jnp.dot(weights, vb, preferred_element_type=F32)
            mixed[t, pl.ds(start, WINDOW), h * HD:(h + 1) * HD] = o.astype(BF16)

    proj_all[t] = proj_ref[...]
    for step in (1, 0):
        spread(*mix_args, step).start()

    def relay_near(m):
        for c in range(CHUNKS):
            hop(m, None, 0, 0, c).wait_recv()
            hop(m, 0, 2, 0, c).start()
            if (m, c) in crossed:
                for j in range(1, groups):
                    cross(m, 0, c, j).start()
            hop(m, None, 1, 0, c).wait_recv()
            for j in range(1, groups):
                cross(m, 1, c, j).start()

    def relay_far(m):
        for c in range(CHUNKS):
            hop(m, 0, 2, 0, c).wait_recv()
            for j in range(1, groups):
                cross(m, 2, c, j).start()

    @pl.when(inner)
    def _():
        relay_near(0)

    for args in (proj_args, mix_args):
        spread_arrival(*args, 1).wait_recv()
        spread(*args, 2).start()
    for args in (proj_args, mix_args):
        for step in (0, 2):
            spread_arrival(*args, step).wait_recv()
    lanes = mixed.shape[2]
    block = summed.shape[0]
    strip = 64

    @pl.loop(0, tokens // block)
    def _(b):
        rows = pl.ds(pl.multiple_of(b * block, block), block)

        @pl.loop(0, tps)
        def _(i):
            at = pl.ds(pl.multiple_of(i * cols, 128), cols)
            prod = jnp.dot(mixed[0, rows, :], proj_all[i, pl.ds(0, lanes), :], preferred_element_type=F32)
            for u in range(1, tps):
                prod += jnp.dot(mixed[u, rows, :], proj_all[i, pl.ds(u * lanes, lanes), :],
                                preferred_element_type=F32)
            summed[:, at] = resid_ref[rows, at].astype(F32) + prod

        @pl.loop(0, block // strip)
        def _(i):
            at = pl.multiple_of(i * strip, strip)
            x = summed[pl.ds(at, strip), :]
            mean = jnp.mean(x, axis=-1, keepdims=True)
            msq = jnp.mean(x * x, axis=-1, keepdims=True)
            normed[pl.ds(pl.multiple_of(base + b * block + at, strip), strip), :] = (
                (x - mean) * lax.rsqrt(msq - mean * mean + 1e-05) * gain_ref[...]
            ).astype(BF16)

    half = width // 2
    my_half = pl.ds(pl.multiple_of(lax.rem(t, 2) * half, half), half)
    peer_half = pl.ds(pl.multiple_of((1 - lax.rem(t, 2)) * half, half), half)

    def norm_in():
        part = normed.at[pl.ds(base, tokens), my_half]
        return remote(part, part, norm_send.at[0], norm_recv.at[0], {"sp": s + inward})

    def norm_in_arrival():
        part = normed.at[pl.ds(other_base, tokens), my_half]
        return remote(part, part, norm_send.at[0], norm_recv.at[0], {"sp": s + inward})

    def norm_over(of_peer):
        part = normed.at[pl.ds(other_base, tokens), peer_half if of_peer else my_half]
        return remote(part, part, norm_send.at[1], norm_recv.at[1], {"tp": core_peer})

    def ret_copy():
        return remote(ret_out, ret_in, ret_send.at[0], ret_recv.at[0], {"sp": s - inward})

    def edge_copy():
        return remote(edge, halo, edge_send.at[0], edge_recv.at[0], {"sp": s + inward})

    half_rows = tokens // 2
    core = lax.rem(t, 2)
    far_first = (1 - t // 2) * 2

    def is_far(p):
        return (p // 2) != (t // 2)

    def half_of(i, c):
        first = (base if i else other_base) + c * half_rows
        return pl.ds(pl.multiple_of(first, half_rows), half_rows)

    def near_copy(i, u):
        rows = pl.ds(base if i else other_base, tokens)
        return remote(terms.at[core_peer, rows], parts.at[u, rows], term_send.at[core_peer, i],
                      term_recv.at[u, i], {"tp": core_peer})

    def pair_copy(p, i):
        return remote(terms.at[p, half_of(i, 1 - core)], pair_in.at[lax.rem(p, 2), i],
                      pair_send.at[lax.rem(p, 2), i], pair_recv.at[lax.rem(p, 2), i], {"tp": core_peer})

    def far_copy(p, i):
        rows = half_of(i, core)
        return remote(terms.at[p, rows], parts.at[t, rows], term_send.at[p, i], term_recv.at[t, i], {"tp": p})

    def far_arrival(c, i):
        u, rows = far_first + c, half_of(i, c)
        return remote(terms.at[u, rows], parts.at[u, rows], term_send.at[u, i], term_recv.at[u, i], {"tp": u})

    tile = 256
    my_cols = pl.ds(pl.multiple_of(t * cols, 128), cols)

    def arrived(m, slot):
        for c in range(CHUNKS):
            for j in range(1, groups):
                if slot == 0 and (m, c) not in crossed:
                    hop(m, None, 0, j, c).wait_recv()
                else:
                    cross_arrival(m, slot, c, j).wait_recv()

    def gate_up(slot):
        if slot is not None:
            arrived(0, slot)
            arrived(1, slot)
        p = s + {None: 0, 0: -1, 1: 1, 2: 2}[slot] * inward

        @pl.loop(0, hidden // tile)
        def _(i):
            at = pl.ds(pl.multiple_of(i * tile, 128), tile)
            x = normed[:, pl.ds(pl.multiple_of(p * depth, 128), depth)]
            wa = wg_ref[:, at] if slot is None else wg_all[slot, :, at]
            ga = jnp.dot(x, wa, preferred_element_type=F32)
            if slot is None:
                gate[pl.ds(PAD, rows2), at] = ga
            else:
                gate[pl.ds(PAD, rows2), at] += ga
            wb = wu_ref[:, at] if slot is None else wu_all[slot, :, at]
            ub = jnp.dot(x, wb, preferred_element_type=F32)
            if slot is None:
                up[:, at] = ub
            else:
                up[:, at] += ub

    def piece_of(slot):
        return s + {None: 0, 0: -1, 1: 1, 2: 2}[slot] * inward

    def down(slot, i):
        if slot is not None and i == 0:
            arrived(2, slot)
        p = piece_of(slot)
        rows = pl.ds(base if i else other_base, tokens)

        @pl.loop(0, cols // tile)
        def _(k):
            at = pl.ds(pl.multiple_of(k * tile, 128), tile)
            w = wd_ref[:, at] if slot is None else wd_all[slot, :, at]
            terms[p, rows, at] = jnp.dot(act[rows, :], w, preferred_element_type=F32).astype(BF16)

        @pl.when(p == core_peer)
        def _():
            near_copy(i, t).start()

        @pl.when(is_far(p))
        def _():
            pair_copy(p, i).start()

    def settle(slot, i):
        p = piece_of(slot)

        @pl.when(is_far(p))
        def _():
            pair_copy(p, i).wait_recv()
            rows = half_of(i, core)
            both = terms[p, rows, :].astype(F32) + pair_in[lax.rem(p, 2), i].astype(F32)
            terms[p, rows, :] = both.astype(BF16)
            far_copy(p, i).start()

    def finish(i, ref):
        near_copy(i, core_peer).wait_recv()
        for c in range(2):
            rows = half_of(i, c)
            out = normed[rows, my_cols].astype(F32) + terms[t, rows, :].astype(F32)
            out = out + parts[core_peer, rows, :].astype(F32)
            far_arrival(c, i).wait_recv()
            out = out + parts[far_first + c, rows, :].astype(F32)
            ref[pl.ds(c * half_rows, half_rows), :] = out.astype(BF16)

    @pl.when(outer)
    def _():
        norm_in().start()
        for m, c, j in direct:
            hop(m, None, 0, j, c).start()
        ret_copy().wait_recv()
        out_ref[...] = ret_in[...]
        norm_in().wait_send()
        for m, c, j in direct:
            hop(m, None, 0, j, c).wait_send()
        for m, c in pieces:
            hop(m, None, 0, 0, c).wait_send()

    @pl.when(inner)
    def _():
        relay_near(1)
        relay_near(2)
        relay_far(0)
        norm_in_arrival().wait_recv()
        norm_over(False).start()
        relay_far(1)
        norm_over(True).wait_recv()
        gate_up(None)
        gate_up(1)
        relay_far(2)
        gate_up(0)
        gate_up(2)

        at_edge = pl.multiple_of(PAD + (1 - s // (n // 2)) * (rows2 - EDGE), PAD)
        edge[...] = gate[pl.ds(at_edge, EDGE), :].astype(BF16)
        edge_copy().start()
        gate[PAD - 1:PAD, :] = jnp.zeros((1, hidden), F32)
        gate[PAD + rows2:PAD + rows2 + 1, :] = jnp.zeros((1, hidden), F32)
        edge_copy().wait_recv()

        @pl.when(low)
        def _():
            gate[PAD + rows2:PAD + rows2 + 1, :] = halo[...].astype(F32)[0:1, :]

        @pl.when(jnp.logical_not(low))
        def _():
            gate[PAD - 1:PAD, :] = halo[...].astype(F32)[EDGE - 1:EDGE, :]

        @pl.loop(0, hidden // 128)
        def _(i):
            at = pl.ds(pl.multiple_of(i * 128, 128), 128)
            gate[pl.ds(PAD, rows2), at] = gate[pl.ds(PAD, rows2), at].astype(BF16).astype(F32)
            conv = cb_ref[:, at]
            for tap in range(CONV):
                conv = conv + gate[pl.ds(PAD - CONV // 2 + tap, rows2), at] * cw_ref[tap:tap + 1, at]
            silu = conv / (1.0 + jnp.exp(-conv))
            act[:, at] = (silu * up[:, at].astype(BF16).astype(F32)).astype(BF16)

        steps = [(slot, i) for i in range(2) for slot in (None, 1, 2, 0)]
        for at, (slot, i) in enumerate(steps):
            down(slot, i)
            if at:
                settle(*steps[at - 1])
        settle(*steps[-1])
        finish(0, ret_out)
        ret_copy().start()
        finish(1, out_ref)

        ret_copy().wait_send()
        edge_copy().wait_send()
        norm_over(False).wait_send()
        for i in range(2):
            near_copy(i, t).wait_send()
            for c in range(2):
                pair_copy(far_first + c, i).wait_send()
                far_copy(far_first + c, i).wait_send()
        for m, c in pieces:
            hop(m, None, 1, 0, c).wait_send()
            hop(m, 0, 2, 0, c).wait_send()
            for j in range(1, groups):
                if (m, c) in crossed:
                    cross(m, 0, c, j).wait_send()
                cross(m, 1, c, j).wait_send()
                cross(m, 2, c, j).wait_send()

    @pl.when(has_left)
    def _():
        for i in range(2):
            halo_copy(i, True).wait_send()

    @pl.when(has_right)
    def _():
        for i in range(2):
            halo_copy(i, False).wait_send()

    for step in range(3):
        spread(*proj_args, step).wait_send()
        spread(*mix_args, step).wait_send()


def kernel_shards(
    sizes, queries, keys, values, sink, resid, out_proj, norm_gain, w_gate, w_up, conv_w, conv_b, w_down
):
    groups, n, tps = sizes
    tokens, width = resid.shape
    cols = out_proj.shape[1]
    depth, hidden = w_gate.shape
    vmem = pl.BlockSpec(memory_space=pltpu.VMEM)
    dma = pltpu.SemaphoreType.DMA
    cross_sems = dma((3, 3, CHUNKS, groups))
    return pl.pallas_call(
        functools.partial(layer_kernel, sizes),
        out_shape=jax.ShapeDtypeStruct((tokens, cols), BF16),
        in_specs=[vmem] * 3 + [pl.BlockSpec(memory_space=pltpu.SMEM)] + [vmem] * 8,
        out_specs=vmem,
        scratch_shapes=[
            pltpu.VMEM((2, tokens + 2 * WINDOW, HD), BF16),
            pltpu.VMEM((tps,) + out_proj.shape, BF16),
            pltpu.VMEM((tps,) + queries.shape, BF16),
            pltpu.VMEM((tokens // 2, width), F32),
            pltpu.VMEM((2 * tokens, width), BF16),
            pltpu.VMEM((n - 1,) + w_gate.shape, BF16),
            pltpu.VMEM((n - 1,) + w_up.shape, BF16),
            pltpu.VMEM((n - 1,) + w_down.shape, BF16),
            pltpu.VMEM((2 * tokens + 2 * PAD, hidden), F32),
            pltpu.VMEM((2 * tokens, hidden), F32),
            pltpu.VMEM((EDGE, hidden), BF16),
            pltpu.VMEM((EDGE, hidden), BF16),
            pltpu.VMEM((2 * tokens, hidden), BF16),
            pltpu.VMEM((tps, 2 * tokens, cols), BF16),
            pltpu.VMEM((tps, 2 * tokens, cols), BF16),
            pltpu.VMEM((2, 2, tokens // 2, cols), BF16),
            pltpu.VMEM((tokens, cols), BF16),
            pltpu.VMEM((tokens, cols), BF16),
            dma((2, 2)), dma((2, 2)),
            dma((3, 3, groups, CHUNKS)), dma((3, 2, groups, CHUNKS)),
            cross_sems, cross_sems,
            dma((3,)), dma((3,)), dma((3,)), dma((3,)), dma((2,)), dma((2,)), dma((1,)), dma((1,)),
            dma((tps, 2)), dma((tps, 2)), dma((2, 2)), dma((2, 2)), dma((1,)), dma((1,)),
        ],
        compiler_params=pltpu.CompilerParams(
            collective_id=0, has_side_effects=True, vmem_limit_bytes=67043328
        ),
    )(queries, keys, values, sink, resid, out_proj, norm_gain[None], w_gate, w_up, conv_w, conv_b[None], w_down)


def fits_kernel(sizes, args):
    groups, n, tps = sizes
    queries, resid, out_proj, w_gate, w_down = args[0], args[4], args[5], args[7], args[11]
    part = groups * CHUNKS * EDGE
    weights = 3 * 2 * n * w_gate.shape[0] * w_gate.shape[1]
    return (
        n == 4
        and tps == 4
        and groups > 1
        and w_down.shape[1] == out_proj.shape[1]
        and w_gate.shape[0] % max(part, 128) == 0
        and w_down.shape[0] % part == 0
        and w_down.shape[1] % 256 == 0
        and w_gate.shape[1] % out_proj.shape[1] == 0
        and resid.shape[0] % (4 * WINDOW) == 0
        and weights <= 20 * 2 ** 20
    )


def run_shards(sizes, *args):
    if fits_kernel(sizes, args):
        return kernel_shards(sizes, *args)
    return shards(*args)


def solution(mesh):
    sizes = tuple(mesh.shape[axis] for axis in ("grp", "sp", "tp"))
    return jax.shard_map(
        functools.partial(run_shards, sizes),
        mesh=mesh,
        in_specs=(
            P(("grp", "sp"), "tp"),
            P(("grp", "sp"), None),
            P(("grp", "sp"), None),
            P("tp"),
            P(("grp", "sp"), None),
            P(None, "tp"),
            P(),
            P("sp", "tp"),
            P("sp", "tp"),
            P(None, "tp"),
            P("tp"),
            P("tp", "sp"),
        ),
        out_specs=P(("grp", "sp"), "tp"),
        check_vma=False,
    )
```

```python
import functools

import jax
import jax.numpy as jnp
from jax import lax
from jax.experimental import pallas as pl
from jax.experimental.pallas import tpu as pltpu
from jax.sharding import PartitionSpec as P

H = 8
KVH = 2
HD = 128
WINDOW = 128
CONV = 3


def with_halo(cells, sides, width):
    for axis, dim in sides:
        count = lax.axis_size(axis)
        ends = count - 1
        head = lax.slice_in_dim(cells, 0, width, axis=dim)
        tail = lax.slice_in_dim(cells, cells.shape[dim] - width, cells.shape[dim], axis=dim)
        cells = jnp.concatenate(
            [
                lax.ppermute(tail, axis, [(i, (i + 1) % count) for i in range(ends)]),
                cells,
                lax.ppermute(head, axis, [((i + 1) % count, i) for i in range(ends)]),
            ],
            axis=dim,
        )
    return cells


def shards(
    queries, keys, values, sink, resid, out_proj, norm_gain, w_gate, w_up, conv_w, conv_b, w_down
):
    tokens = queries.shape[0]
    width = resid.shape[1]
    heads_here = sink.shape[0]
    group = H // KVH
    scale = HD ** (-0.5)
    first_head = lax.axis_index("tp") * heads_here
    kv_head = first_head // group
    own_keys = lax.dynamic_slice_in_dim(keys, kv_head * HD, HD, 1)
    own_values = lax.dynamic_slice_in_dim(values, kv_head * HD, HD, 1)
    extended = with_halo(jnp.stack([own_keys, own_values]), (("sp", 1),), WINDOW)
    ext_keys = extended[0]
    ext_values = extended[1]
    span = tokens + 2 * WINDOW
    q_heads = queries.reshape(tokens, heads_here, HD)
    scores = (
        jnp.einsum("qhd,kd->hqk", q_heads, ext_keys, preferred_element_type=jnp.float32) * scale
    )
    offset = lax.axis_index("sp") * tokens
    q_pos = offset + jnp.arange(tokens, dtype=jnp.int32)[:, None]
    k_pos = offset - WINDOW + jnp.arange(span, dtype=jnp.int32)[None, :]
    seq_total = tokens * lax.axis_size("sp")
    valid = (jnp.abs(q_pos - k_pos) <= WINDOW) & (k_pos >= 0) & (k_pos < seq_total)
    scores = jnp.where(valid[None], scores, jnp.float32(-1e30))
    sink_col = sink[:, None]
    top = jnp.maximum(jnp.max(scores, axis=-1), sink_col)
    expo = jnp.exp(scores - top[..., None])
    total = jnp.sum(expo, axis=-1) + jnp.exp(sink_col - top)
    weights = (expo / total[..., None]).astype(jnp.bfloat16)
    heads_out = jnp.einsum("hqk,kd->qhd", weights, ext_values, preferred_element_type=jnp.float32)
    heads_out = heads_out.astype(jnp.bfloat16).reshape(tokens, heads_here * HD)
    all_heads = lax.all_gather(heads_out, "tp", axis=1, tiled=True)
    cols = width // lax.axis_size("tp")
    col_start = lax.axis_index("tp") * cols
    full_proj = lax.all_gather(out_proj, "tp", axis=1, tiled=True)
    summed = resid.astype(jnp.float32) + jnp.dot(
        all_heads, full_proj, preferred_element_type=jnp.float32
    )
    mean = jnp.mean(summed, axis=-1, keepdims=True)
    msq = jnp.mean(summed * summed, axis=-1, keepdims=True)
    normed_full = ((summed - mean) * lax.rsqrt(msq - mean * mean + 1e-05) * norm_gain).astype(
        jnp.bfloat16
    )
    normed_own = lax.dynamic_slice_in_dim(normed_full, col_start, cols, 1)
    gate_acc = jnp.dot(
        normed_full,
        lax.all_gather(w_gate, "sp", axis=0, tiled=True),
        preferred_element_type=jnp.float32,
    )
    up_acc = jnp.dot(
        normed_full,
        lax.all_gather(w_up, "sp", axis=0, tiled=True),
        preferred_element_type=jnp.float32,
    )
    gate_pre = gate_acc.astype(jnp.bfloat16)
    up_part = up_acc.astype(jnp.bfloat16)
    padded = with_halo(gate_pre, (("sp", 0),), CONV // 2)
    conv = conv_b
    for tap in range(CONV):
        conv = conv + padded[tap : tap + tokens].astype(jnp.float32) * conv_w[tap]
    act = (jax.nn.silu(conv) * up_part.astype(jnp.float32)).astype(jnp.bfloat16)
    terms = jnp.dot(
        act, lax.all_gather(w_down, "sp", axis=1, tiled=True), preferred_element_type=jnp.float32
    )
    ffn_own = lax.psum_scatter(
        terms.astype(jnp.bfloat16), "tp", scatter_dimension=1, tiled=True
    ).astype(jnp.float32)
    return (normed_own.astype(jnp.float32) + ffn_own).astype(jnp.bfloat16)


CHUNKS = 2
CROSSED = 1
PAD = 8
EDGE = 16
BF16 = jnp.bfloat16
F32 = jnp.float32


def layer_kernel(
    sizes,
    q_ref, k_ref, v_ref, sink_ref, resid_ref, proj_ref, gain_ref, wg_ref, wu_ref, cw_ref, cb_ref, wd_ref,
    out_ref,
    kv_ext, proj_all, mixed, summed, normed, wg_all, wu_all, wd_all, gate, up, edge, halo, act, terms, parts,
    pair_in, ret_out, ret_in,
    halo_send, halo_recv, z_recv, z_send, y_recv, y_send,
    proj_send, proj_recv, mix_send, mix_recv, norm_send, norm_recv, edge_send, edge_recv,
    term_send, term_recv, pair_send, pair_recv, ret_send, ret_recv,
):
    groups, n, tps = sizes
    g = lax.axis_index("grp")
    s = lax.axis_index("sp")
    t = lax.axis_index("tp")
    tokens, width = resid_ref.shape
    heads_here = sink_ref.shape[0]
    cols = proj_ref.shape[1]
    depth = wg_ref.shape[0]
    hidden = wg_ref.shape[1]
    rows2 = 2 * tokens
    has_left, has_right = s > 0, s < n - 1
    inner = has_left & has_right
    outer = jnp.logical_not(inner)
    low = s < n // 2
    inward = 1 - 2 * (s // (n // 2))
    base = pl.multiple_of(lax.rem(s, 2) * tokens, tokens)
    other_base = pl.multiple_of((1 - lax.rem(s, 2)) * tokens, tokens)
    core_peer = t + 1 - 2 * lax.rem(t, 2)
    chip_peer = lax.rem(t + 2, tps)
    own = (wg_ref, wu_ref, wd_ref)
    full = (wg_all, wu_all, wd_all)

    def remote(src, dst, send, recv, to):
        return pltpu.make_async_remote_copy(
            src_ref=src, dst_ref=dst, send_sem=send, recv_sem=recv,
            device_id=to, device_id_type=pl.DeviceIdType.MESH,
        )

    barrier = pltpu.get_barrier_semaphore()

    def greet(to):
        pl.semaphore_signal(barrier, inc=1, device_id=to, device_id_type=pl.DeviceIdType.MESH)

    @pl.when(has_left)
    def _():
        greet({"sp": s - 1})

    @pl.when(has_right)
    def _():
        greet({"sp": s + 1})

    for j in range(1, groups):
        greet({"grp": lax.rem(g + j, groups)})
    for j in range(1, tps):
        greet({"tp": lax.rem(t + j, tps)})
    along = jnp.minimum(s, 1) + jnp.minimum(n - 1 - s, 1)
    pl.semaphore_wait(barrier, along + groups - 1 + tps - 1)

    kv_head = (t * heads_here) // (H // KVH)
    kv_cols = pl.ds(pl.multiple_of(kv_head * HD, HD), HD)

    def halo_copy(i, to_left):
        ref = (k_ref, v_ref)[i]
        if to_left:
            return remote(ref.at[pl.ds(0, WINDOW), kv_cols], kv_ext.at[i, pl.ds(WINDOW + tokens, WINDOW)],
                          halo_send.at[i, 0], halo_recv.at[i, 0], {"sp": s - 1})
        return remote(ref.at[pl.ds(tokens - WINDOW, WINDOW), kv_cols], kv_ext.at[i, pl.ds(0, WINDOW)],
                      halo_send.at[i, 1], halo_recv.at[i, 1], {"sp": s + 1})

    def rows_of(m, part, c):
        step = own[m].shape[0] // (groups * CHUNKS)
        return pl.ds(pl.multiple_of((part * CHUNKS + c) * step, EDGE), step)

    def hop(m, src_slot, dst_slot, j, c):
        part = lax.rem(g + j, groups)
        rows = rows_of(m, part, c)
        src = own[m].at[rows] if src_slot is None else full[m].at[src_slot, rows]
        return remote(src, full[m].at[dst_slot, rows], z_send.at[m, 0 if src_slot is None else 1, j, c],
                      z_recv.at[m, dst_slot, j, c], {"sp": s + inward})

    def cross(m, slot, c, j):
        rows = rows_of(m, g, c)
        return remote(full[m].at[slot, rows], full[m].at[slot, rows], y_send.at[m, slot, c, j],
                      y_recv.at[m, slot, c, j], {"grp": lax.rem(g + j, groups)})

    def cross_arrival(m, slot, c, j):
        rows = rows_of(m, lax.rem(g + groups - j, groups), c)
        return remote(full[m].at[slot, rows], full[m].at[slot, rows], y_send.at[m, slot, c, j],
                      y_recv.at[m, slot, c, j], {"grp": lax.rem(g + j, groups)})

    pieces = [(m, c) for m in range(3) for c in range(CHUNKS)]
    crossed = pieces[:CROSSED]
    direct = [(m, c, j) for m, c in pieces[CROSSED:] for j in range(1, groups)]

    def spread(src, ref, send, recv, step):
        origin = (t, t, chip_peer)[step]
        return remote(src if step < 2 else ref.at[origin], ref.at[origin], send.at[step], recv.at[step],
                      {"tp": (core_peer, chip_peer, core_peer)[step]})

    def spread_arrival(src, ref, send, recv, step):
        origin = (core_peer, chip_peer, lax.rem(core_peer + 2, tps))[step]
        return remote(src, ref.at[origin], send.at[step], recv.at[step],
                      {"tp": (core_peer, chip_peer, core_peer)[step]})

    proj_args = (proj_ref, proj_all, proj_send, proj_recv)
    mix_args = (mixed.at[t], mixed, mix_send, mix_recv)

    @pl.when(has_left)
    def _():
        for i in range(2):
            halo_copy(i, True).start()

    @pl.when(has_right)
    def _():
        for i in range(2):
            halo_copy(i, False).start()

    @pl.when(outer)
    def _():
        for m, c in pieces:
            hop(m, None, 0, 0, c).start()

    @pl.when(inner)
    def _():
        for m, c in pieces[:2 * CHUNKS]:
            hop(m, None, 1, 0, c).start()

    for step in (1, 0):
        spread(*proj_args, step).start()

    for i, ref in enumerate((k_ref, v_ref)):
        kv_ext[i, pl.ds(WINDOW, tokens), :] = ref[:, kv_cols]

    @pl.when(jnp.logical_not(has_left))
    def _():
        kv_ext[:, pl.ds(0, WINDOW), :] = jnp.zeros((2, WINDOW, HD), BF16)

    @pl.when(jnp.logical_not(has_right))
    def _():
        kv_ext[:, pl.ds(WINDOW + tokens, WINDOW), :] = jnp.zeros((2, WINDOW, HD), BF16)

    @pl.when(has_right)
    def _():
        for i in range(2):
            halo_copy(i, True).wait_recv()

    @pl.when(has_left)
    def _():
        for i in range(2):
            halo_copy(i, False).wait_recv()

    span = 3 * WINDOW
    seq_total = tokens * n

    @pl.loop(0, tokens // WINDOW)
    def _(b):
        start = pl.multiple_of(b * WINDOW, WINDOW)
        row = lax.broadcasted_iota(jnp.int32, (WINDOW, span), 0)
        col = lax.broadcasted_iota(jnp.int32, (WINDOW, span), 1)
        k_pos = s * tokens + start - WINDOW + col
        valid = (jnp.abs(row + WINDOW - col) <= WINDOW) & (k_pos >= 0) & (k_pos < seq_total)
        kb = kv_ext[0, pl.ds(start, span), :]
        vb = kv_ext[1, pl.ds(start, span), :]
        for h in range(heads_here):
            qb = q_ref[pl.ds(start, WINDOW), h * HD:(h + 1) * HD]
            sc = lax.dot_general(qb, kb, (((1,), (1,)), ((), ())), preferred_element_type=F32) * (HD ** -0.5)
            sc = jnp.where(valid, sc, F32(-1e30))
            sink = sink_ref[h]
            top = jnp.maximum(jnp.max(sc, axis=-1, keepdims=True), sink)
            expo = jnp.exp(sc - top)
            total = jnp.sum(expo, axis=-1, keepdims=True) + jnp.exp(sink - top)
            weights = (expo / total).astype(BF16)
            o = jnp.dot(weights, vb, preferred_element_type=F32)
            mixed[t, pl.ds(start, WINDOW), h * HD:(h + 1) * HD] = o.astype(BF16)

    proj_all[t] = proj_ref[...]
    for step in (1, 0):
        spread(*mix_args, step).start()

    def relay_near(m):
        for c in range(CHUNKS):
            hop(m, None, 0, 0, c).wait_recv()
            hop(m, 0, 2, 0, c).start()
            if (m, c) in crossed:
                for j in range(1, groups):
                    cross(m, 0, c, j).start()
            hop(m, None, 1, 0, c).wait_recv()
            for j in range(1, groups):
                cross(m, 1, c, j).start()

    def relay_far(m):
        for c in range(CHUNKS):
            hop(m, 0, 2, 0, c).wait_recv()
            for j in range(1, groups):
                cross(m, 2, c, j).start()

    @pl.when(inner)
    def _():
        relay_near(0)

    for args in (proj_args, mix_args):
        spread_arrival(*args, 1).wait_recv()
        spread(*args, 2).start()
    for args in (proj_args, mix_args):
        for step in (0, 2):
            spread_arrival(*args, step).wait_recv()
    lanes = mixed.shape[2]
    block = summed.shape[0]
    strip = 64

    @pl.loop(0, tokens // block)
    def _(b):
        rows = pl.ds(pl.multiple_of(b * block, block), block)

        @pl.loop(0, tps)
        def _(i):
            at = pl.ds(pl.multiple_of(i * cols, 128), cols)
            prod = jnp.dot(mixed[0, rows, :], proj_all[i, pl.ds(0, lanes), :], preferred_element_type=F32)
            for u in range(1, tps):
                prod += jnp.dot(mixed[u, rows, :], proj_all[i, pl.ds(u * lanes, lanes), :],
                                preferred_element_type=F32)
            summed[:, at] = resid_ref[rows, at].astype(F32) + prod

        @pl.loop(0, block // strip)
        def _(i):
            at = pl.multiple_of(i * strip, strip)
            x = summed[pl.ds(at, strip), :]
            mean = jnp.mean(x, axis=-1, keepdims=True)
            msq = jnp.mean(x * x, axis=-1, keepdims=True)
            normed[pl.ds(pl.multiple_of(base + b * block + at, strip), strip), :] = (
                (x - mean) * lax.rsqrt(msq - mean * mean + 1e-05) * gain_ref[...]
            ).astype(BF16)

    half = width // 2
    my_half = pl.ds(pl.multiple_of(lax.rem(t, 2) * half, half), half)
    peer_half = pl.ds(pl.multiple_of((1 - lax.rem(t, 2)) * half, half), half)

    def norm_in():
        part = normed.at[pl.ds(base, tokens), my_half]
        return remote(part, part, norm_send.at[0], norm_recv.at[0], {"sp": s + inward})

    def norm_in_arrival():
        part = normed.at[pl.ds(other_base, tokens), my_half]
        return remote(part, part, norm_send.at[0], norm_recv.at[0], {"sp": s + inward})

    def norm_over(of_peer):
        part = normed.at[pl.ds(other_base, tokens), peer_half if of_peer else my_half]
        return remote(part, part, norm_send.at[1], norm_recv.at[1], {"tp": core_peer})

    def ret_copy():
        return remote(ret_out, ret_in, ret_send.at[0], ret_recv.at[0], {"sp": s - inward})

    def edge_copy():
        return remote(edge, halo, edge_send.at[0], edge_recv.at[0], {"sp": s + inward})

    half_rows = tokens // 2
    core = lax.rem(t, 2)
    far_first = (1 - t // 2) * 2

    def is_far(p):
        return (p // 2) != (t // 2)

    def half_of(i, c):
        first = (base if i else other_base) + c * half_rows
        return pl.ds(pl.multiple_of(first, half_rows), half_rows)

    def near_copy(i, u):
        rows = pl.ds(base if i else other_base, tokens)
        return remote(terms.at[core_peer, rows], parts.at[u, rows], term_send.at[core_peer, i],
                      term_recv.at[u, i], {"tp": core_peer})

    def pair_copy(p, i):
        return remote(terms.at[p, half_of(i, 1 - core)], pair_in.at[lax.rem(p, 2), i],
                      pair_send.at[lax.rem(p, 2), i], pair_recv.at[lax.rem(p, 2), i], {"tp": core_peer})

    def far_copy(p, i):
        rows = half_of(i, core)
        return remote(terms.at[p, rows], parts.at[t, rows], term_send.at[p, i], term_recv.at[t, i], {"tp": p})

    def far_arrival(c, i):
        u, rows = far_first + c, half_of(i, c)
        return remote(terms.at[u, rows], parts.at[u, rows], term_send.at[u, i], term_recv.at[u, i], {"tp": u})

    tile = 256
    my_cols = pl.ds(pl.multiple_of(t * cols, 128), cols)

    def arrived(m, slot):
        for c in range(CHUNKS):
            for j in range(1, groups):
                if slot == 0 and (m, c) not in crossed:
                    hop(m, None, 0, j, c).wait_recv()
                else:
                    cross_arrival(m, slot, c, j).wait_recv()

    def gate_up(slot):
        if slot is not None:
            arrived(0, slot)
            arrived(1, slot)
        p = s + {None: 0, 0: -1, 1: 1, 2: 2}[slot] * inward

        @pl.loop(0, hidden // tile)
        def _(i):
            at = pl.ds(pl.multiple_of(i * tile, 128), tile)
            x = normed[:, pl.ds(pl.multiple_of(p * depth, 128), depth)]
            wa = wg_ref[:, at] if slot is None else wg_all[slot, :, at]
            ga = jnp.dot(x, wa, preferred_element_type=F32)
            if slot is None:
                gate[pl.ds(PAD, rows2), at] = ga
            else:
                gate[pl.ds(PAD, rows2), at] += ga
            wb = wu_ref[:, at] if slot is None else wu_all[slot, :, at]
            ub = jnp.dot(x, wb, preferred_element_type=F32)
            if slot is None:
                up[:, at] = ub
            else:
                up[:, at] += ub

    def piece_of(slot):
        return s + {None: 0, 0: -1, 1: 1, 2: 2}[slot] * inward

    def down(slot, i):
        if slot is not None and i == 0:
            arrived(2, slot)
        p = piece_of(slot)
        rows = pl.ds(base if i else other_base, tokens)

        @pl.loop(0, cols // tile)
        def _(k):
            at = pl.ds(pl.multiple_of(k * tile, 128), tile)
            w = wd_ref[:, at] if slot is None else wd_all[slot, :, at]
            terms[p, rows, at] = jnp.dot(act[rows, :], w, preferred_element_type=F32).astype(BF16)

        @pl.when(p == core_peer)
        def _():
            near_copy(i, t).start()

        @pl.when(is_far(p))
        def _():
            pair_copy(p, i).start()

    def settle(slot, i):
        p = piece_of(slot)

        @pl.when(is_far(p))
        def _():
            pair_copy(p, i).wait_recv()
            rows = half_of(i, core)
            both = terms[p, rows, :].astype(F32) + pair_in[lax.rem(p, 2), i].astype(F32)
            terms[p, rows, :] = both.astype(BF16)
            far_copy(p, i).start()

    def finish(i, ref):
        near_copy(i, core_peer).wait_recv()
        for c in range(2):
            rows = half_of(i, c)
            out = normed[rows, my_cols].astype(F32) + terms[t, rows, :].astype(F32)
            out = out + parts[core_peer, rows, :].astype(F32)
            far_arrival(c, i).wait_recv()
            out = out + parts[far_first + c, rows, :].astype(F32)
            ref[pl.ds(c * half_rows, half_rows), :] = out.astype(BF16)

    @pl.when(outer)
    def _():
        norm_in().start()
        for m, c, j in direct:
            hop(m, None, 0, j, c).start()
        ret_copy().wait_recv()
        out_ref[...] = ret_in[...]
        norm_in().wait_send()
        for m, c, j in direct:
            hop(m, None, 0, j, c).wait_send()
        for m, c in pieces:
            hop(m, None, 0, 0, c).wait_send()

    @pl.when(inner)
    def _():
        relay_near(1)
        for m, c in pieces[2 * CHUNKS:]:
            hop(m, None, 1, 0, c).start()
        relay_far(0)
        relay_far(1)
        norm_in_arrival().wait_recv()
        norm_over(False).start()
        relay_near(2)
        norm_over(True).wait_recv()
        gate_up(None)
        gate_up(1)
        gate_up(2)
        relay_far(2)
        gate_up(0)

        at_edge = pl.multiple_of(PAD + (1 - s // (n // 2)) * (rows2 - EDGE), PAD)
        edge[...] = gate[pl.ds(at_edge, EDGE), :].astype(BF16)
        edge_copy().start()
        gate[PAD - 1:PAD, :] = jnp.zeros((1, hidden), F32)
        gate[PAD + rows2:PAD + rows2 + 1, :] = jnp.zeros((1, hidden), F32)
        edge_copy().wait_recv()

        @pl.when(low)
        def _():
            gate[PAD + rows2:PAD + rows2 + 1, :] = halo[...].astype(F32)[0:1, :]

        @pl.when(jnp.logical_not(low))
        def _():
            gate[PAD - 1:PAD, :] = halo[...].astype(F32)[EDGE - 1:EDGE, :]

        @pl.loop(0, hidden // 128)
        def _(i):
            at = pl.ds(pl.multiple_of(i * 128, 128), 128)
            gate[pl.ds(PAD, rows2), at] = gate[pl.ds(PAD, rows2), at].astype(BF16).astype(F32)
            conv = cb_ref[:, at]
            for tap in range(CONV):
                conv = conv + gate[pl.ds(PAD - CONV // 2 + tap, rows2), at] * cw_ref[tap:tap + 1, at]
            silu = conv / (1.0 + jnp.exp(-conv))
            act[:, at] = (silu * up[:, at].astype(BF16).astype(F32)).astype(BF16)

        steps = [(slot, i) for slots in ((None, 1), (0, 2)) for i in range(2) for slot in slots]
        for at, (slot, i) in enumerate(steps):
            down(slot, i)
            if at:
                settle(*steps[at - 1])
        settle(*steps[-1])
        finish(0, ret_out)
        ret_copy().start()
        finish(1, out_ref)

        ret_copy().wait_send()
        edge_copy().wait_send()
        norm_over(False).wait_send()
        for i in range(2):
            near_copy(i, t).wait_send()
            for c in range(2):
                pair_copy(far_first + c, i).wait_send()
                far_copy(far_first + c, i).wait_send()
        for m, c in pieces:
            hop(m, None, 1, 0, c).wait_send()
            hop(m, 0, 2, 0, c).wait_send()
            for j in range(1, groups):
                if (m, c) in crossed:
                    cross(m, 0, c, j).wait_send()
                cross(m, 1, c, j).wait_send()
                cross(m, 2, c, j).wait_send()

    @pl.when(has_left)
    def _():
        for i in range(2):
            halo_copy(i, True).wait_send()

    @pl.when(has_right)
    def _():
        for i in range(2):
            halo_copy(i, False).wait_send()

    for step in range(3):
        spread(*proj_args, step).wait_send()
        spread(*mix_args, step).wait_send()


def kernel_shards(
    sizes, queries, keys, values, sink, resid, out_proj, norm_gain, w_gate, w_up, conv_w, conv_b, w_down
):
    groups, n, tps = sizes
    tokens, width = resid.shape
    cols = out_proj.shape[1]
    depth, hidden = w_gate.shape
    vmem = pl.BlockSpec(memory_space=pltpu.VMEM)
    dma = pltpu.SemaphoreType.DMA
    cross_sems = dma((3, 3, CHUNKS, groups))
    return pl.pallas_call(
        functools.partial(layer_kernel, sizes),
        out_shape=jax.ShapeDtypeStruct((tokens, cols), BF16),
        in_specs=[vmem] * 3 + [pl.BlockSpec(memory_space=pltpu.SMEM)] + [vmem] * 8,
        out_specs=vmem,
        scratch_shapes=[
            pltpu.VMEM((2, tokens + 2 * WINDOW, HD), BF16),
            pltpu.VMEM((tps,) + out_proj.shape, BF16),
            pltpu.VMEM((tps,) + queries.shape, BF16),
            pltpu.VMEM((tokens // 2, width), F32),
            pltpu.VMEM((2 * tokens, width), BF16),
            pltpu.VMEM((n - 1,) + w_gate.shape, BF16),
            pltpu.VMEM((n - 1,) + w_up.shape, BF16),
            pltpu.VMEM((n - 1,) + w_down.shape, BF16),
            pltpu.VMEM((2 * tokens + 2 * PAD, hidden), F32),
            pltpu.VMEM((2 * tokens, hidden), F32),
            pltpu.VMEM((EDGE, hidden), BF16),
            pltpu.VMEM((EDGE, hidden), BF16),
            pltpu.VMEM((2 * tokens, hidden), BF16),
            pltpu.VMEM((tps, 2 * tokens, cols), BF16),
            pltpu.VMEM((tps, 2 * tokens, cols), BF16),
            pltpu.VMEM((2, 2, tokens // 2, cols), BF16),
            pltpu.VMEM((tokens, cols), BF16),
            pltpu.VMEM((tokens, cols), BF16),
            dma((2, 2)), dma((2, 2)),
            dma((3, 3, groups, CHUNKS)), dma((3, 2, groups, CHUNKS)),
            cross_sems, cross_sems,
            dma((3,)), dma((3,)), dma((3,)), dma((3,)), dma((2,)), dma((2,)), dma((1,)), dma((1,)),
            dma((tps, 2)), dma((tps, 2)), dma((2, 2)), dma((2, 2)), dma((1,)), dma((1,)),
        ],
        compiler_params=pltpu.CompilerParams(
            collective_id=0, has_side_effects=True, vmem_limit_bytes=67043328
        ),
    )(queries, keys, values, sink, resid, out_proj, norm_gain[None], w_gate, w_up, conv_w, conv_b[None], w_down)


def fits_kernel(sizes, args):
    groups, n, tps = sizes
    queries, resid, out_proj, w_gate, w_down = args[0], args[4], args[5], args[7], args[11]
    part = groups * CHUNKS * EDGE
    weights = 3 * 2 * n * w_gate.shape[0] * w_gate.shape[1]
    return (
        n == 4
        and tps == 4
        and groups > 1
        and w_down.shape[1] == out_proj.shape[1]
        and w_gate.shape[0] % max(part, 128) == 0
        and w_down.shape[0] % part == 0
        and w_down.shape[1] % 256 == 0
        and w_gate.shape[1] % out_proj.shape[1] == 0
        and resid.shape[0] % (4 * WINDOW) == 0
        and weights <= 20 * 2 ** 20
    )


def run_shards(sizes, *args):
    if fits_kernel(sizes, args):
        return kernel_shards(sizes, *args)
    return shards(*args)


def solution(mesh):
    sizes = tuple(mesh.shape[axis] for axis in ("grp", "sp", "tp"))
    return jax.shard_map(
        functools.partial(run_shards, sizes),
        mesh=mesh,
        in_specs=(
            P(("grp", "sp"), "tp"),
            P(("grp", "sp"), None),
            P(("grp", "sp"), None),
            P("tp"),
            P(("grp", "sp"), None),
            P(None, "tp"),
            P(),
            P("sp", "tp"),
            P("sp", "tp"),
            P(None, "tp"),
            P("tp"),
            P("tp", "sp"),
        ),
        out_specs=P(("grp", "sp"), "tp"),
        check_vma=False,
    )
```
